128 devices in a mesh: sp: 16 (over z, y), tp: 8 (over x, core).
Axes of the slice: x: 4, y: 4, z: 4, core: 2. Of those that a mesh axis runs over, the one named last changes fastest.
Arguments:
- stream: bfloat16 [6144, 2048], P(('sp', 'tp')), may hold values from -6 to 6
- query_nope: bfloat16 [6144, 16, 128], P('sp', 'tp'), may hold values from -6 to 6
- query_rope: bfloat16 [6144, 16, 64], P('sp', 'tp'), may hold values from -700 to 700
- latent: bfloat16 [6144, 512], P('sp'), may hold values from -6 to 6
- rope_key: bfloat16 [6144, 64], P('sp'), may hold values from -6 to 6
- latent_gain: float32 [512], replicated, may hold values from 0.1 to 1.9
- key_up: bfloat16 [512, 16, 128], P(None, 'tp'), may hold values from -0.375 to 0.375
- value_up: bfloat16 [512, 16, 128], P(None, 'tp'), may hold values from -2.6516504 to 2.6516504
- out_gain: float32 [2048], P('tp'), may hold values from 0.1 to 1.9
- out_weight: bfloat16 [2048, 2048], P('tp'), may hold values from -0.125 to 0.125
- norm_gain: float32 [2048], replicated, may hold values from 0.1 to 1.9
- ff_in: bfloat16 [2048, 8192], P('sp', 'tp'), may hold values from -0.125 to 0.125
- ff_out: bfloat16 [8192, 2048], P('tp', 'sp'), may hold values from -0.0625 to 0.0625
Outputs:
- layer_out: bfloat16 [6144, 2048], P(('sp', 'tp'))
The draws below stay inside these ranges and needn't reach their ends.
All inputs are finite; a program needn't handle non-finite values.
Results may differ from the reference program's by a relative error of at most 0.018.
Values may be sent and summed in bfloat16 or wider, within the bound.
A program may use at most 128 MiB of HBM per device.

```python
import math
import jax
import jax.numpy as jnp
from jax import lax

D = 2048
FF = 8192
HEADS = 16
NOPE = 128
ROPE = 64
LATENT = 512
VDIM = 128
TOKENS = 6144


def draw_query_rope(key, part):
    base_draw = jax.random.normal(key, (TOKENS, HEADS, ROPE), jnp.float32)
    return jnp.clip(base_draw, -700.0, 700.0).astype(jnp.bfloat16)


def draw_value_up(key, part):
    base_draw = jnp.clip(jax.random.normal(key, (LATENT, HEADS, VDIM), jnp.float32), -6.0, 6.0) / jnp.sqrt(jnp.float32(LATENT))
    factor = jnp.power(4.0, jnp.arange(HEADS, dtype=jnp.float32) / max(HEADS - 1, 1))
    return (base_draw * factor[None, :, None]).astype(jnp.bfloat16)


def block_levels(rng, extent, split, low, largest):
    def one(axis_at, blocks):
        heights = jax.random.uniform(jax.random.fold_in(jax.random.fold_in(rng, 6), axis_at), (blocks,), jnp.float32, low / len(split), largest / len(split))
        return jnp.repeat(jnp.exp(heights), extent[axis_at] // blocks).reshape((-1,) + (1,) * (len(extent) - axis_at - 1))

    level = one(*split[0])
    for cut in split[1:]:
        level = level * one(*cut)
    return level


def scatter_about(key, shape, scale, reach, split=(), kind=jnp.bfloat16):
    entries = scale * jax.random.normal(key, shape, jnp.float32)
    if split:
        entries = entries * block_levels(key, shape, split, -0.22, 0.18)
    return jnp.clip(entries, -reach, reach).astype(kind)


def setup_inputs(seed: int = 0) -> dict:
    key_list = jax.random.split(jax.random.key(seed), 14)
    stream = scatter_about(key_list[0], (TOKENS, D), 1.0, 6.0, ((0, 128),))
    query_nope = scatter_about(key_list[1], (TOKENS, HEADS, NOPE), 1.0, 6.0, ((0, 16), (1, 8)))
    query_rope = draw_query_rope(jax.random.fold_in(key_list[13], 71), 0)
    latent = scatter_about(key_list[3], (TOKENS, LATENT), 1.0, 6.0, ((0, 16),))
    rope_key = scatter_about(key_list[4], (TOKENS, ROPE), 1.0, 6.0, ((0, 16),))
    latent_gain = jnp.clip(1.0 + 0.18 * jax.random.normal(key_list[5], (LATENT,), jnp.float32), 0.1, 1.9)
    key_up = scatter_about(key_list[6], (LATENT, HEADS, NOPE), (2 * NOPE) ** -0.5, 0.375, ((1, 8),))
    value_up = draw_value_up(jax.random.fold_in(key_list[13], 71), 0)
    out_gain = jnp.clip(1.0 + 0.18 * jax.random.normal(key_list[8], (HEADS * VDIM,), jnp.float32), 0.1, 1.9)
    out_weight = scatter_about(key_list[9], (HEADS * VDIM, D), (HEADS * VDIM) ** -0.5, 0.125, ((0, 8),))
    norm_gain = jnp.clip(1.0 + 0.18 * jax.random.normal(key_list[10], (D,), jnp.float32), 0.1, 1.9)
    ff_in = scatter_about(key_list[11], (D, FF), D ** -0.5, 0.125, ((0, 16), (1, 8)))
    ff_out = scatter_about(key_list[12], (FF, D), FF ** -0.5, 0.0625, ((0, 8), (1, 16)))
    return {"stream": stream, "query_nope": query_nope, "query_rope": query_rope, "latent": latent, "rope_key": rope_key, "latent_gain": latent_gain, "key_up": key_up, "value_up": value_up, "out_gain": out_gain, "out_weight": out_weight, "norm_gain": norm_gain, "ff_in": ff_in, "ff_out": ff_out}


EPS = 1e-06
THETA = 10000.0

def turn(values, positions):
    full_width = values.shape[-1]
    half_width = full_width // 2
    inverse = jnp.power(THETA, -jnp.arange(0, full_width, 2, dtype=jnp.float32) / full_width)
    angles = positions[:, None] * inverse[None, :]
    cosine = jnp.cos(angles)
    sine_part = jnp.sin(angles)
    if values.ndim == 3:
        cosine = cosine[:, None, :]
        sine_part = sine_part[:, None, :]
    vector = values.astype(jnp.float32)
    lower_half = vector[..., :half_width]
    upper_half = vector[..., half_width:]
    return jnp.concatenate([lower_half * cosine - upper_half * sine_part, lower_half * sine_part + upper_half * cosine], axis=-1)

def reference(stream, query_nope, query_rope, latent, rope_key, latent_gain, key_up, value_up, out_gain, out_weight, norm_gain, ff_in, ff_out):
    positions = jnp.arange(TOKENS, dtype=jnp.float32)
    lat_full = latent.astype(jnp.float32)
    normed = (lat_full * lax.rsqrt(lax.optimization_barrier(jnp.mean(lat_full * lat_full, axis=-1, keepdims=True)) + EPS) * latent_gain.astype(jnp.float32)).astype(jnp.bfloat16)
    keys_rot = turn(rope_key, positions).astype(jnp.bfloat16)
    query_rot = turn(query_rope, positions).astype(jnp.bfloat16)
    query_lat = jnp.einsum('thn,lhn->thl', query_nope.astype(jnp.float32), key_up.astype(jnp.float32)).astype(jnp.bfloat16)
    score_scale = 1.0 / math.sqrt(NOPE + ROPE)
    normed_wide = normed.astype(jnp.float32)
    keys_wide = keys_rot.astype(jnp.float32)

    def attend(inputs):
        lat_query, rot_query = inputs
        scores = (jnp.einsum('thl,kl->thk', lat_query.astype(jnp.float32), normed_wide) + jnp.einsum('thr,kr->thk', rot_query.astype(jnp.float32), keys_wide)) * score_scale
        row_max = lax.optimization_barrier(jnp.max(scores, axis=-1, keepdims=True))
        expo = jnp.exp(scores - row_max)
        denom = lax.optimization_barrier(jnp.sum(expo, axis=-1))
        probs = lax.optimization_barrier(expo.astype(jnp.bfloat16)).astype(jnp.float32)
        summed = jnp.einsum('thk,kl->thl', probs, normed_wide)
        return (summed / denom[..., None]).astype(jnp.bfloat16)
    q_block = math.gcd(TOKENS, 512)
    out_lat = lax.map(attend, (query_lat.reshape(TOKENS // q_block, q_block, HEADS, LATENT), query_rot.reshape(TOKENS // q_block, q_block, HEADS, ROPE)))
    out_lat = out_lat.reshape(TOKENS, HEADS, LATENT)
    head_out = jnp.einsum('thl,lhv->thv', out_lat.astype(jnp.float32), value_up.astype(jnp.float32))
    row_scale = lax.rsqrt(lax.optimization_barrier(jnp.mean(head_out * head_out, axis=(1, 2))) + EPS)
    gated = (head_out.reshape(TOKENS, HEADS * VDIM) * out_gain.astype(jnp.float32)).astype(jnp.bfloat16)
    mid_stream = stream.astype(jnp.float32) + row_scale[:, None] * jnp.dot(gated, out_weight, preferred_element_type=jnp.float32)
    ff_input = (mid_stream * lax.rsqrt(lax.optimization_barrier(jnp.mean(mid_stream * mid_stream, axis=-1, keepdims=True)) + EPS) * norm_gain.astype(jnp.float32)).astype(jnp.bfloat16)
    pre_act = jnp.dot(ff_input, ff_in, preferred_element_type=jnp.float32)
    activation = jnp.square(jax.nn.relu(pre_act)).astype(jnp.bfloat16)
    return (mid_stream + jnp.dot(activation, ff_out, preferred_element_type=jnp.float32)).astype(jnp.bfloat16)
```

```python
import math

import jax
import jax.numpy as jnp
import numpy as np
from jax import lax
from jax.experimental import pallas as pl
from jax.experimental.pallas import tpu as pltpu
from jax.sharding import PartitionSpec as P

MESH = pl.DeviceIdType.MESH
F32 = jnp.float32
BF16 = jnp.bfloat16

HEADS = 16
NOPE = 128
ROPE = 64
LATENT = 512
VDIM = 128
EPS = 1e-06
THETA = 10000.0

SIDE = 4
BLOCKS = SIDE * SIDE
ROWS = 384
OWN = 48
D = 2048
HID = 1024
PACK = 1152
PAIR = ROWS // 2
EXT = D + 128
UNIT = 4 * PAIR

YP, YM, ZP, ZM = (1, 0), (-1, 0), (0, 1), (0, -1)
LINKS = (YP, YM, ZP, ZM)


def wrap(v):
    return ((v[0] + 4) % 4, (v[1] + 4) % 4)


class Msg:
    def __init__(self, d, e, part, parent):
        self.d, self.e, self.part, self.parent = d, wrap(e), part, parent
        self.f = wrap((e[0] - d[0], e[1] - d[1]))
        self.level = 1 if parent is None else parent.level + 1
        self.kids = []
        self.id = None


def forwards(m):
    alongy = m.d[1] == 0
    first, cross = ("H0", (ZP, ZM)) if alongy else ("H1", (YP, YM))
    plus = m.d in (YP, ZP)
    out = []
    if m.part == "all":
        if plus:
            out.append((m.d, "a"))
        else:
            out += [(m.d, "H0b"), (m.d, "H1b")]
        out += [(c, first) for c in cross]
    elif m.level == 2 and m.part == "a":
        out += [(c, first + "a") for c in cross]
    elif m.level == 2 and m.part == first + "b":
        out += [(c, first + "b") for c in cross]
    elif m.level == 2 and m.part in ("H0", "H1"):
        out.append((m.d, m.part + ("a" if plus else "b")))
    elif m.level == 3 and m.parent.parent is not None and m.parent.level == 2 and m.parent.d != m.d:
        if m.part[2] == ("a" if plus else "b"):
            out.append((m.d, m.part))
    return out


def build_messages():
    todo = [Msg(d, (0, 0), "all", None) for d in LINKS]
    done = []
    while todo:
        m = todo.pop(0)
        m.id = len(done)
        done.append(m)
        m.kids = [Msg(d, m.f, part, m) for d, part in forwards(m)]
        todo += m.kids
    return done


MSGS = build_messages()
NMSG = len(MSGS)
LEVELS = [[m for m in MSGS if m.level == k] for k in (1, 2, 3, 4)]
ORDER = [(0, 0)]
_seen = {(0, 0): 4}
_quarters = {"all": "ABCD", "H0": "AB", "H1": "CD", "a": "BC", "H0b": "A", "H0a": "B", "H1a": "C", "H1b": "D"}
LAST = {}
for _m in MSGS:
    _seen[_m.f] = _seen.get(_m.f, 0) + len(_quarters[_m.part])
    if _seen[_m.f] == 4:
        ORDER.append(_m.f)
        LAST[_m.id] = _m.f
assert len(ORDER) == BLOCKS and all(v == 4 for v in _seen.values())
SLOT = {f: k for k, f in enumerate(ORDER)}


def parts_of(a, b, c, d):
    total = a + b + c + d
    return {
        "all": (0, total),
        "H0": (0, a + b),
        "H1": (a + b, c + d),
        "a": (a, b + c),
        "H0b": (0, a),
        "H0a": (a, b),
        "H1a": (a + b, c),
        "H1b": (a + b + c, d),
    }


LAT_PARTS = parts_of(16, 32, 16, 32)
IN_PARTS = parts_of(32, 32, 32, 32)
OUT_PARTS = parts_of(256, 256, 256, 256)


def rotary_tables():
    half = ROPE // 2
    inverse = np.power(THETA, -np.arange(0, ROPE, 2, dtype=np.float64) / ROPE)
    base = inverse[:, None] * np.arange(ROWS)[None, :]
    start = inverse[None, :] * (ROWS * np.arange(BLOCKS))[:, None]
    near = np.concatenate([np.cos(base), np.sin(base)], 0).astype(np.float32)
    far = np.concatenate([np.cos(start), np.sin(start)], 1).astype(np.float32)
    far = np.repeat(far[:, :, None], 128, axis=2)
    assert far.shape == (BLOCKS, 2 * half, 128)
    return near, far


def kernel(
    stream_in,
    qn,
    qr_t,
    latent,
    kr_t,
    lat_gain,
    key_up,
    value_up,
    out_gain,
    out_w_in,
    norm_gain,
    ff_in,
    ff_out,
    near,
    far_in,
    out,
    cat,
    w1,
    w2,
    qa,
    qb,
    sa,
    sb,
    pa,
    pb,
    acc,
    m_run,
    l_run,
    far,
    stream,
    out_w,
    proj,
    sib,
    xs,
    rx,
    fin,
    act,
    part,
    psib,
    pxs,
    prx,
    mid,
    fsum,
    loc_sem,
    ls,
    lr,
    s1,
    r1,
    s2,
    r2,
    ds,
    dr,
    ps,
    pr,
    fs,
    fr,
    gs,
    gr,
):
    sp = lax.axis_index("sp")
    tp = lax.axis_index("tp")
    z, y = sp // SIDE, sp % SIDE
    x, core = tp // 2, tp % 2
    other = 1 - core

    def at(f):
        return ((z + f[1]) % SIDE) * SIDE + (y + f[0]) % SIDE

    def torus(d):
        return (at(d), tp)

    sibling = (sp, x * 2 + other)

    def across(k):
        return (sp, ((x + k) % SIDE) * 2 + core)

    barrier = pltpu.get_barrier_semaphore()
    peers = [torus(d) for d in LINKS] + [sibling] + [across(k) for k in (1, 2, 3)]
    for peer in peers:
        pl.semaphore_signal(barrier, inc=1, device_id=peer, device_id_type=MESH)

    def local(src, dst, k):
        c = pltpu.make_async_copy(src, dst, loc_sem.at[k])
        c.start()
        return c

    far_copy = local(far_in.at[sp], far, 0)
    w1_copy = local(ff_in, w1.at[sp], 1)
    w2_copy = local(ff_out, w2.at[sp], 2)
    ow_copy = local(out_w_in, out_w, 3)
    st_copy = local(stream_in, stream, 4)

    def remote(src, dst, ssem, rsem, dev):
        return pltpu.make_async_remote_copy(
            src_ref=src, dst_ref=dst, send_sem=ssem, recv_sem=rsem, device_id=dev, device_id_type=MESH
        )

    def lat_view(f, part_name, whose):
        first, count = LAT_PARTS[part_name]
        start = SLOT[f] * PAIR + first + whose * (PAIR // 2)
        return cat.at[pl.ds(pl.multiple_of(start, 16), count), :]

    def lat_src(f, p):
        return lat_view(f, p, core)

    def in_view(f, p):
        first, count = IN_PARTS[p]
        return w1.at[at(f), pl.ds(first, count), :]

    def in_src(f, p):
        return ff_in if f == (0, 0) else in_view(f, p)

    def out_view(f, p):
        first, count = OUT_PARTS[p]
        return w2.at[at(f), pl.ds(first, count), :]

    def out_src(f, p):
        return ff_out if f == (0, 0) else out_view(f, p)

    gathers = {
        "L": (lat_src, lat_src, ls, lr),
        "W1": (in_src, in_view, s1, r1),
        "W2": (out_src, out_view, s2, r2),
    }

    def copy_of(g, m):
        src, view, ssem, rsem = gathers[g]
        if g == "L":
            first, count = LAT_PARTS[m.part]
            start = SLOT[m.f] * PAIR + first + core * (PAIR // 2)
            dst = cat.at[pl.ds(pl.multiple_of(start, 16), count), :]
        else:
            dst = view(m.e, m.part)
        return remote(src(m.e, m.part), dst, ssem.at[m.id], rsem.at[m.id], torus(m.d))

    def share(f):
        v = cat.at[pl.ds(pl.multiple_of(SLOT[f] * PAIR + core * (PAIR // 2), 32), PAIR // 2), :]
        return remote(v, v, ds.at[SLOT[f]], dr.at[SLOT[f]], sibling)

    def shared(f):
        v = cat.at[pl.ds(pl.multiple_of(SLOT[f] * PAIR + other * (PAIR // 2), 32), PAIR // 2), :]
        remote(v, v, ds.at[SLOT[f]], dr.at[SLOT[f]], sibling).wait_recv()

    def begin(g):
        for m in LEVELS[0]:
            copy_of(g, m).start()

    def receive(g, m):
        _, view, ssem, rsem = gathers[g]
        v = view(m.f, m.part)
        remote(v, v, ssem.at[m.id], rsem.at[m.id], torus(m.d)).wait_recv()
        for k in m.kids:
            copy_of(g, k).start()
        if g == "L" and m.id in LAST:
            share(LAST[m.id]).start()

    def level(g, k):
        for m in LEVELS[k - 1]:
            receive(g, m)

    lat = latent[...].astype(F32)
    normed = (
        lat * lax.rsqrt(jnp.mean(lat * lat, axis=-1, keepdims=True) + EPS) * lat_gain[...]
    ).astype(BF16)
    cat[0:PAIR, 0:LATENT] = normed[:PAIR]
    cat[0:PAIR, LATENT + 128 : PACK] = normed[PAIR:]
    far_copy.wait()
    half = ROPE // 2
    cos_n, sin_n = near[0:half, :], near[half:ROPE, :]
    cos_f = jnp.broadcast_to(far[0:half, 0:1], (half, ROWS))
    sin_f = jnp.broadcast_to(far[half:ROPE, 0:1], (half, ROWS))
    cosine = cos_n * cos_f - sin_n * sin_f
    sine = sin_n * cos_f + cos_n * sin_f

    def turned(v):
        low, high = v[:half].astype(F32), v[half:].astype(F32)
        a = low * cosine - high * sine
        b = low * sine + high * cosine
        return jnp.transpose(jnp.concatenate([a, b, a, b], axis=0))

    lane = lax.broadcasted_iota(jnp.int32, (ROWS, 128), 1)
    keys = turned(kr_t[...])
    cat[0:PAIR, LATENT : LATENT + 128] = jnp.where(
        lane[:PAIR] < ROPE, keys[:PAIR], keys[PAIR:]
    ).astype(BF16)

    pl.semaphore_wait(barrier, len(peers))
    begin("L")
    begin("W1")

    for h in range(2):
        rows = slice(h * ROWS, (h + 1) * ROWS)
        q_lat = lax.dot_general(
            qn[:, h * NOPE : (h + 1) * NOPE],
            key_up[:, h * NOPE : (h + 1) * NOPE],
            (((1,), (1,)), ((), ())),
            preferred_element_type=F32,
        ).astype(BF16)
        q_rot = turned(qr_t[h])
        qa[rows, 0:LATENT] = q_lat
        qa[rows, LATENT : LATENT + 128] = jnp.where(lane < ROPE, q_rot, 0.0).astype(BF16)
        qb[rows, 128 : LATENT + 128] = q_lat
        qb[rows, 0:128] = jnp.where(lane < ROPE, 0.0, q_rot).astype(BF16)

    acc[...] = jnp.zeros_like(acc)
    m_run[...] = jnp.full_like(m_run, -1e30)
    l_run[...] = jnp.zeros_like(l_run)
    factor = math.log2(math.e) / math.sqrt(NOPE + ROPE)

    def score(q, s, first):
        return lax.dot_general(
            q[...],
            cat[s * UNIT : (s + 1) * UNIT, first : first + LATENT + 128],
            (((1,), (1,)), ((), ())),
            preferred_element_type=F32,
        )

    def weigh(s_ref, p_ref, s, first):
        scores = s_ref[...]
        before = m_run[...]
        now = jnp.maximum(before, jnp.max(scores, axis=1, keepdims=True) * factor)
        fade = jnp.exp2(before - now)
        total = l_run[...] * fade
        for k in range(UNIT // 128):
            expo = jnp.exp2(scores[:, k * 128 : (k + 1) * 128] * factor - now)
            total = total + expo
            p_ref[:, k * 128 : (k + 1) * 128] = expo.astype(BF16)
        l_run[...] = total
        m_run[...] = now
        mixed = jnp.dot(
            p_ref[...],
            cat[s * UNIT : (s + 1) * UNIT, first : first + LATENT],
            preferred_element_type=F32,
        )
        for k in range(LATENT // 128):
            c = slice(k * 128, (k + 1) * 128)
            acc[:, c] = acc[:, c] * fade + mixed[:, c]

    def attend(s):
        sa[...] = score(qa, s, 0)
        sb[...] = score(qb, s, LATENT)
        weigh(sa, pa, s, 0)
        weigh(sb, pb, s, LATENT + 128)

    def need(first, last):
        for f in ORDER[first:last]:
            shared(f)

    level("L", 1)
    need(1, 4)
    attend(0)
    level("L", 2)
    level("W1", 1)
    need(4, 8)
    attend(1)
    level("L", 3)
    begin("W2")
    need(8, 12)
    attend(2)
    level("L", 4)
    level("W1", 2)
    need(12, 16)
    attend(3)
    level("W1", 3)

    out_lat = (acc[...] / jnp.sum(l_run[...], axis=1, keepdims=True)).astype(BF16)
    squares = jnp.zeros((ROWS, 1), F32)
    gated = []
    for h in range(2):
        c = slice(h * VDIM, (h + 1) * VDIM)
        head_out = jnp.dot(
            out_lat[h * ROWS : (h + 1) * ROWS], value_up[:, c], preferred_element_type=F32
        )
        squares = squares + jnp.sum(head_out * head_out, axis=1, keepdims=True)
        gated.append((head_out * out_gain[:, c]).astype(BF16))
    gated = jnp.concatenate(gated, axis=1)

    def two_terms(total, rows):
        high = total.astype(BF16).astype(F32)
        at_lane = lax.broadcasted_iota(jnp.int32, (rows, 128), 1)
        return jnp.where(at_lane == 0, high, jnp.where(at_lane == 1, total - high, 0.0)).astype(BF16)

    ow_copy.wait()
    tail = two_terms(squares, ROWS)
    for c in range(0, D, 512):
        piece = jnp.dot(gated, out_w[:, c : c + 512], preferred_element_type=F32).astype(BF16)
        proj[:, :, :, c : c + 512] = piece.reshape(SIDE, 2, OWN, 512)
    proj[:, :, :, D:EXT] = tail.reshape(SIDE, 2, OWN, 128)

    swap = remote(proj.at[:, other], sib, ps.at[0], pr.at[0], sibling)
    swap.start()
    swap.wait_recv()
    sends = [swap]

    def chip_sum(k):
        who = (x + k) % SIDE
        both = proj[who, core].astype(F32) + sib[who].astype(F32)
        total = jnp.sum(both[:, D:EXT], axis=1, keepdims=True)
        return both[:, :D], total

    for k in (1, 3, 2):
        body, total = chip_sum(k)
        xs[k - 1, :, 0:D] = body.astype(BF16)
        xs[k - 1, :, D:EXT] = two_terms(total, OWN)
        c = remote(xs.at[k - 1], rx.at[k - 1], ps.at[k], pr.at[k], across(k))
        c.start()
        sends.append(c)
    projected, total = chip_sum(0)
    level("W1", 4)
    level("W2", 1)
    for k in (1, 3, 2):
        remote(rx.at[k - 1], rx.at[k - 1], ps.at[k], pr.at[k], across(k)).wait_recv()
        projected = projected + rx[k - 1, :, 0:D].astype(F32)
        total = total + jnp.sum(rx[k - 1, :, D:EXT].astype(F32), axis=1, keepdims=True)
    row_scale = lax.rsqrt(total / (HEADS * VDIM) + EPS)
    st_copy.wait()
    middle = stream[...].astype(F32) + row_scale * projected
    mid[...] = middle
    ff_row = (
        middle
        * lax.rsqrt(jnp.mean(middle * middle, axis=-1, keepdims=True) + EPS)
        * norm_gain[...]
    ).astype(BF16)
    fin[tp] = ff_row

    def row_copy(k, to, src_tp):
        v = fin.at[src_tp]
        return remote(v, v, fs.at[k], fr.at[k], to)

    for k in (1, 3, 2):
        c = row_copy(k, across(k), tp)
        c.start()
        sends.append(c)
    c = row_copy(0, sibling, tp)
    c.start()
    sends.append(c)
    level("W2", 2)
    for k in (1, 3, 2):
        came = ((x + SIDE - k) % SIDE) * 2
        row_copy(k, across(k), came + core).wait_recv()
        c = row_copy(3 + k, sibling, came + core)
        c.start()
        sends.append(c)
    row_copy(0, sibling, x * 2 + other).wait_recv()
    for k in (1, 3, 2):
        came = ((x + SIDE - k) % SIDE) * 2
        row_copy(3 + k, sibling, came + other).wait_recv()

    w1_copy.wait()
    w2_copy.wait()
    rows = fin[...].reshape(ROWS, D)
    for c in range(0, HID, 256):
        pre = jnp.dot(
            rows, w1[:, :, c : c + 256].reshape(D, 256), preferred_element_type=F32
        )
        act[:, c : c + 256] = jnp.square(jnp.maximum(pre, 0.0)).astype(BF16)

    def swap_part(g):
        return remote(part.at[g, :, other], psib.at[g], gs.at[g, 0], gr.at[g, 0], sibling)

    def x_part(g, k):
        return remote(pxs.at[g, k - 1], prx.at[g, k - 1], gs.at[g, k], gr.at[g, k], across(k))

    def ff_group(g):
        for n, f in enumerate(ORDER[4 * g : 4 * g + 4]):
            piece = jnp.dot(act[...], w2[at(f)], preferred_element_type=F32).astype(BF16)
            part[g, :, :, :, n * 128 : (n + 1) * 128] = piece.reshape(SIDE, 2, OWN, 128)
        swap_part(g).start()

    def ff_chip(g):
        swap_part(g).wait_recv()
        for k in (1, 3, 2, 0):
            who = (x + k) % SIDE
            both = part[g, who, core].astype(F32) + psib[g, who].astype(F32)
            if k:
                pxs[g, k - 1] = both.astype(BF16)
                x_part(g, k).start()
            else:
                fsum[g] = both

    def ff_end(g):
        both = fsum[g]
        for k in (1, 3, 2):
            x_part(g, k).wait_recv()
            both = both + prx[g, k - 1].astype(F32)
        for n, f in enumerate(ORDER[4 * g : 4 * g + 4]):
            c = pl.ds(pl.multiple_of(at(f) * 128, 128), 128)
            out[:, c] = (mid[:, c] + both[:, n * 128 : (n + 1) * 128]).astype(BF16)

    ff_group(0)
    level("W2", 3)
    ff_group(1)
    ff_chip(0)
    level("W2", 4)
    ff_group(2)
    ff_chip(1)
    ff_group(3)
    ff_chip(2)
    ff_end(0)
    ff_chip(3)
    ff_end(1)
    ff_end(2)
    ff_end(3)

    for g in ("L", "W1", "W2"):
        for m in MSGS:
            copy_of(g, m).wait_send()
    for f in ORDER[1:]:
        share(f).wait_send()
    for c in sends:
        c.wait_send()
    for g in range(4):
        swap_part(g).wait_send()
        for k in (1, 2, 3):
            x_part(g, k).wait_send()


def body(
    stream,
    query_nope,
    query_rope,
    latent,
    rope_key,
    latent_gain,
    key_up,
    value_up,
    out_gain,
    out_weight,
    norm_gain,
    ff_in,
    ff_out,
):
    near, far = rotary_tables()
    vmem = pl.BlockSpec(memory_space=pltpu.VMEM)
    hbm = pl.BlockSpec(memory_space=pl.ANY)
    dma = pltpu.SemaphoreType.DMA
    return pl.pallas_call(
        kernel,
        out_shape=jax.ShapeDtypeStruct((OWN, D), BF16),
        in_specs=[hbm, vmem, vmem, vmem, vmem, vmem, vmem, vmem, vmem, hbm, vmem, hbm, hbm, vmem, hbm],
        out_specs=vmem,
        scratch_shapes=[
            pltpu.VMEM((BLOCKS * PAIR, PACK), BF16),
            pltpu.VMEM((BLOCKS, D // BLOCKS, HID), BF16),
            pltpu.VMEM((BLOCKS, HID, D // BLOCKS), BF16),
            pltpu.VMEM((2 * ROWS, LATENT + 128), BF16),
            pltpu.VMEM((2 * ROWS, LATENT + 128), BF16),
            pltpu.VMEM((2 * ROWS, UNIT), F32),
            pltpu.VMEM((2 * ROWS, UNIT), F32),
            pltpu.VMEM((2 * ROWS, UNIT), BF16),
            pltpu.VMEM((2 * ROWS, UNIT), BF16),
            pltpu.VMEM((2 * ROWS, LATENT), F32),
            pltpu.VMEM((2 * ROWS, 128), F32),
            pltpu.VMEM((2 * ROWS, 128), F32),
            pltpu.VMEM((ROPE, 128), F32),
            pltpu.VMEM((OWN, D), BF16),
            pltpu.VMEM((2 * VDIM, D), BF16),
            pltpu.VMEM((SIDE, 2, OWN, EXT), BF16),
            pltpu.VMEM((SIDE, OWN, EXT), BF16),
            pltpu.VMEM((SIDE - 1, OWN, EXT), BF16),
            pltpu.VMEM((SIDE - 1, OWN, EXT), BF16),
            pltpu.VMEM((2 * SIDE, OWN, D), BF16),
            pltpu.VMEM((ROWS, HID), BF16),
            pltpu.VMEM((4, SIDE, 2, OWN, 512), BF16),
            pltpu.VMEM((4, SIDE, OWN, 512), BF16),
            pltpu.VMEM((4, SIDE - 1, OWN, 512), BF16),
            pltpu.VMEM((4, SIDE - 1, OWN, 512), BF16),
            pltpu.VMEM((OWN, D), F32),
            pltpu.VMEM((4, OWN, 512), F32),
            dma((5,)),
            dma((NMSG,)),
            dma((NMSG,)),
            dma((NMSG,)),
            dma((NMSG,)),
            dma((NMSG,)),
            dma((NMSG,)),
            dma((BLOCKS,)),
            dma((BLOCKS,)),
            dma((4,)),
            dma((4,)),
            dma((7,)),
            dma((7,)),
            dma((4, 4)),
            dma((4, 4)),
        ],
        compiler_params=pltpu.CompilerParams(
            collective_id=0, has_side_effects=True, vmem_limit_bytes=60 * 1024 * 1024
        ),
    )(
        stream,
        query_nope.reshape(ROWS, 2 * NOPE),
        jnp.transpose(query_rope, (1, 2, 0)),
        latent,
        jnp.transpose(rope_key, (1, 0)),
        latent_gain.reshape(1, LATENT),
        key_up.reshape(LATENT, 2 * NOPE),
        value_up.reshape(LATENT, 2 * VDIM),
        out_gain.reshape(1, 2 * VDIM),
        out_weight,
        norm_gain.reshape(1, D),
        ff_in,
        ff_out,
        jnp.asarray(near),
        jnp.asarray(far),
    )


def solution(mesh):
    placed = (
        P(("sp", "tp"), None),
        P("sp", "tp", None),
        P("sp", "tp", None),
        P("sp", None),
        P("sp", None),
        P(),
        P(None, "tp", None),
        P(None, "tp", None),
        P("tp"),
        P("tp", None),
        P(),
        P("sp", "tp"),
        P("tp", "sp"),
    )
    return jax.shard_map(
        body, mesh=mesh, in_specs=placed, out_specs=P(("sp", "tp"), None), check_vma=False
    )
```

```python
import math

import jax
import jax.numpy as jnp
import numpy as np
from jax import lax
from jax.experimental import pallas as pl
from jax.experimental.pallas import tpu as pltpu
from jax.sharding import PartitionSpec as P

MESH = pl.DeviceIdType.MESH
F32 = jnp.float32
BF16 = jnp.bfloat16

HEADS = 16
NOPE = 128
ROPE = 64
LATENT = 512
VDIM = 128
EPS = 1e-06
THETA = 10000.0

SIDE = 4
BLOCKS = SIDE * SIDE
ROWS = 384
OWN = 48
D = 2048
HID = 1024
PACK = 1152
PAIR = ROWS // 2
EXT = D + 128
UNIT = 4 * PAIR

UP, UM, VP, VM = (1, 0), (-1, 0), (0, 1), (0, -1)
LINKS = (UP, UM, VP, VM)


def wrap(v):
    return ((v[0] + 4) % 4, (v[1] + 4) % 4)


class Msg:
    def __init__(self, d, e, part, parent):
        self.d, self.e, self.part = d, wrap(e), part
        self.f = wrap((e[0] - d[0], e[1] - d[1]))
        self.level = 1 if parent is None else parent.level + 1
        self.kids = []
        self.id = None


def forwards(m):
    plus = m.d in (UP, VP)
    half = "a" if plus else "b"
    if m.d[1] == 0:
        across = [(VP, m.part), (VM, m.part)]
        return ([(m.d, half)] if m.part == "all" else []) + across
    if m.f[1] == 2 or m.part not in ("all", half):
        return []
    return [(m.d, half)]


def build_messages():
    todo = [Msg(d, (0, 0), "all", None) for d in LINKS]
    done = []
    while todo:
        m = todo.pop(0)
        m.id = len(done)
        done.append(m)
        m.kids = [Msg(d, m.f, part, m) for d, part in forwards(m)]
        todo += m.kids
    return done


MSGS = build_messages()
NMSG = len(MSGS)
LEVELS = [[m for m in MSGS if m.level == k] for k in (1, 2, 3, 4)]
ORDER = [(0, 0)]
_seen = {(0, 0): 2}
LAST = {}
for _m in MSGS:
    _seen[_m.f] = _seen.get(_m.f, 0) + (2 if _m.part == "all" else 1)
    if _seen[_m.f] == 2:
        ORDER.append(_m.f)
        LAST[_m.id] = _m.f
assert len(ORDER) == BLOCKS and all(v == 2 for v in _seen.values())
SLOT = {f: k for k, f in enumerate(ORDER)}
SLOTS_AT = [[SLOT[LAST[m.id]] for m in lev if m.id in LAST] for lev in LEVELS]
COLUMNS = ORDER


def parts_of(a, b):
    return {"all": (0, a + b), "a": (0, a), "b": (a, b)}


LAT_PARTS = parts_of(32, 32)
IN_PARTS = parts_of(64, 64)
OUT_PARTS = parts_of(512, 512)
THIRD = 32


def rotary_tables():
    half = ROPE // 2
    inverse = np.power(THETA, -np.arange(0, ROPE, 2, dtype=np.float64) / ROPE)
    base = inverse[:, None] * np.arange(ROWS)[None, :]
    start = inverse[None, :] * (ROWS * np.arange(BLOCKS))[:, None]
    near = np.concatenate([np.cos(base), np.sin(base)], 0).astype(np.float32)
    far = np.concatenate([np.cos(start), np.sin(start)], 1).astype(np.float32)
    far = np.repeat(far[:, :, None], 128, axis=2)
    assert far.shape == (BLOCKS, 2 * half, 128)
    return near, far


def kernel(
    stream_in,
    qn_in,
    qr_in,
    latent_in,
    kr_in,
    lat_gain,
    key_up_in,
    value_up_in,
    out_gain,
    out_w_in,
    norm_gain,
    ff_in,
    ff_out,
    near_in,
    far_in,
    out,
    qn,
    qr_t,
    latent,
    kr_t,
    key_up,
    value_up,
    near,
    cat,
    w1,
    w2,
    qa,
    qb,
    sa,
    sb,
    pa,
    pb,
    acc,
    m_run,
    l_run,
    far,
    stream,
    out_w,
    proj,
    sib,
    xs,
    rx,
    fin,
    act,
    part,
    psib,
    pxs,
    prx,
    mid,
    fsum,
    wide,
    wide2,
    xls,
    xlr,
    loc_sem,
    ls,
    lr,
    s1,
    r1,
    s2,
    r2,
    ds,
    dr,
    ps,
    pr,
    fs,
    fr,
    gs,
    gr,
):
    sp = lax.axis_index("sp")
    tp = lax.axis_index("tp")
    z, y = sp // SIDE, sp % SIDE
    x, core = tp // 2, tp % 2
    other = 1 - core

    odd = x % 2

    def block_at(dy, dz):
        return ((z + dz) % SIDE) * SIDE + (y + dy) % SIDE

    def at(f):
        return block_at(f[0] * other + f[1] * core, f[0] * core + f[1] * other)

    def torus(d):
        return (at(wrap(d)), tp)

    sibling = (sp, x * 2 + other)

    def across(k):
        return (sp, ((x + k) % SIDE) * 2 + core)

    barrier = pltpu.get_barrier_semaphore()
    peers = [torus(d) for d in LINKS] + [sibling] + [across(k) for k in (1, 2, 3)]
    for peer in peers:
        pl.semaphore_signal(barrier, inc=1, device_id=peer, device_id_type=MESH)

    def local(src, dst, k):
        c = pltpu.make_async_copy(src, dst, loc_sem.at[k])
        c.start()
        return c

    early = [
        local(latent_in, latent, 5),
        local(far_in.at[sp], far, 0),
        local(near_in, near, 6),
        local(kr_in, kr_t, 7),
    ]
    early2 = [local(qn_in, qn, 8), local(key_up_in, key_up, 9), local(qr_in, qr_t, 10)]
    vu_copy = local(value_up_in, value_up, 11)
    w1_copy = local(ff_in, w1.at[sp], 1)
    w2_copy = local(ff_out, w2.at[sp], 2)
    ow_copy = local(out_w_in, out_w, 3)
    st_copy = local(stream_in, stream, 4)

    def remote(src, dst, ssem, rsem, dev):
        return pltpu.make_async_remote_copy(
            src_ref=src, dst_ref=dst, send_sem=ssem, recv_sem=rsem, device_id=dev, device_id_type=MESH
        )

    def lat_rows(slot, first, count):
        return cat.at[pl.ds(pl.multiple_of(slot * PAIR + first, 32), count), :]

    def lat_view(f, part_name):
        first, count = LAT_PARTS[part_name]
        return lat_rows(SLOT[f], core * (PAIR // 2) + odd * THIRD + first, count)

    def in_view(f, p):
        first, count = IN_PARTS[p]
        return w1.at[at(f), pl.ds(first, count), :]

    def in_src(f, p):
        return ff_in if f == (0, 0) else in_view(f, p)

    def out_view(f, p):
        first, count = OUT_PARTS[p]
        return w2.at[at(f), pl.ds(first, count), :]

    def out_src(f, p):
        return ff_out if f == (0, 0) else out_view(f, p)

    gathers = {
        "L": (lat_view, lat_view, ls, lr),
        "W1": (in_src, in_view, s1, r1),
        "W2": (out_src, out_view, s2, r2),
    }

    def copy_of(g, m):
        src, view, ssem, rsem = gathers[g]
        dst = view(m.f if g == "L" else m.e, m.part)
        return remote(src(m.e, m.part), dst, ssem.at[m.id], rsem.at[m.id], torus(m.d))

    def along_x(slot):
        v = lat_rows(slot, core * (PAIR // 2) + odd * 2 * THIRD, THIRD)
        return remote(v, v, xls.at[slot], xlr.at[slot], across(1 if slot % 2 == 0 else 3))

    def share(slot):
        v = lat_rows(slot, core * (PAIR // 2), PAIR // 2)
        return remote(v, v, ds.at[slot], dr.at[slot], sibling)

    def pass_over(slots):
        for slot in slots:
            v = lat_rows(slot, core * (PAIR // 2) + (1 - odd) * 2 * THIRD, THIRD)
            remote(v, v, xls.at[slot], xlr.at[slot], sibling).wait_recv()
            share(slot).start()

    def need(slots):
        for slot in slots:
            v = lat_rows(slot, other * (PAIR // 2), PAIR // 2)
            remote(v, v, ds.at[slot], dr.at[slot], sibling).wait_recv()

    def begin(g):
        for m in LEVELS[0]:
            copy_of(g, m).start()

    def receive(g, m):
        _, view, ssem, rsem = gathers[g]
        v = view(m.f, m.part)
        remote(v, v, ssem.at[m.id], rsem.at[m.id], torus(m.d)).wait_recv()
        for k in m.kids:
            copy_of(g, k).start()
        if g == "L" and m.id in LAST:
            along_x(SLOT[LAST[m.id]]).start()

    def level(g, k):
        for m in LEVELS[k - 1]:
            receive(g, m)

    for c in early:
        c.wait()
    lat = latent[...].astype(F32)
    normed = (
        lat * lax.rsqrt(jnp.mean(lat * lat, axis=-1, keepdims=True) + EPS) * lat_gain[...]
    ).astype(BF16)
    cat[0:PAIR, 0:LATENT] = normed[:PAIR]
    cat[0:PAIR, LATENT + 128 : PACK] = normed[PAIR:]
    half = ROPE // 2
    cos_n, sin_n = near[0:half, :], near[half:ROPE, :]
    cos_f = jnp.broadcast_to(far[0:half, 0:1], (half, ROWS))
    sin_f = jnp.broadcast_to(far[half:ROPE, 0:1], (half, ROWS))
    cosine = cos_n * cos_f - sin_n * sin_f
    sine = sin_n * cos_f + cos_n * sin_f

    def turned(v):
        low, high = v[:half].astype(F32), v[half:].astype(F32)
        a = low * cosine - high * sine
        b = low * sine + high * cosine
        return jnp.transpose(jnp.concatenate([a, b, a, b], axis=0))

    lane = lax.broadcasted_iota(jnp.int32, (ROWS, 128), 1)
    keys = turned(kr_t[...])
    cat[0:PAIR, LATENT : LATENT + 128] = jnp.where(
        lane[:PAIR] < ROPE, keys[:PAIR], keys[PAIR:]
    ).astype(BF16)

    pl.semaphore_wait(barrier, len(peers))
    begin("L")

    for c in early2:
        c.wait()
    wide[0 : 2 * ROWS, :] = qn[...].astype(F32)
    wide2[...] = key_up[...].astype(F32)
    for h in range(2):
        rows = slice(h * ROWS, (h + 1) * ROWS)
        q_lat = lax.dot_general(
            wide[pl.ds(h, ROWS, stride=2), :].astype(BF16),
            wide2[pl.ds(h, LATENT, stride=2), :].astype(BF16),
            (((1,), (1,)), ((), ())),
            preferred_element_type=F32,
        ).astype(BF16)
        q_rot = turned(qr_t[h])
        qa[rows, 0:LATENT] = q_lat
        qa[rows, LATENT : LATENT + 128] = jnp.where(lane < ROPE, q_rot, 0.0).astype(BF16)
        qb[rows, 128 : LATENT + 128] = q_lat
        qb[rows, 0:128] = jnp.where(lane < ROPE, 0.0, q_rot).astype(BF16)

    acc[...] = jnp.zeros_like(acc)
    m_run[...] = jnp.full_like(m_run, -1e30)
    l_run[...] = jnp.zeros_like(l_run)
    factor = math.log2(math.e) / math.sqrt(NOPE + ROPE)

    def score(q, first_slot, slots, first):
        return lax.dot_general(
            q[...],
            cat[first_slot * PAIR : (first_slot + slots) * PAIR, first : first + LATENT + 128],
            (((1,), (1,)), ((), ())),
            preferred_element_type=F32,
        )

    def weigh(s_ref, p_ref, first_slot, slots, first):
        keys_here = slots * PAIR
        scores = s_ref[:, 0:keys_here]
        before = m_run[...]
        now = jnp.maximum(before, jnp.max(scores, axis=1, keepdims=True) * factor)
        fade = jnp.exp2(before - now)
        total = l_run[...] * fade
        for k in range(keys_here // 128):
            expo = jnp.exp2(scores[:, k * 128 : (k + 1) * 128] * factor - now)
            total = total + expo
            p_ref[:, k * 128 : (k + 1) * 128] = expo.astype(BF16)
        l_run[...] = total
        m_run[...] = now
        mixed = jnp.dot(
            p_ref[:, 0:keys_here],
            cat[first_slot * PAIR : (first_slot + slots) * PAIR, first : first + LATENT],
            preferred_element_type=F32,
        )
        for k in range(LATENT // 128):
            c = slice(k * 128, (k + 1) * 128)
            acc[:, c] = acc[:, c] * fade + mixed[:, c]

    def attend(first_slot, slots):
        keys_here = slots * PAIR
        sa[:, 0:keys_here] = score(qa, first_slot, slots, 0)
        sb[:, 0:keys_here] = score(qb, first_slot, slots, LATENT)
        weigh(sa, pa, first_slot, slots, 0)
        weigh(sb, pb, first_slot, slots, LATENT + 128)

    level("L", 1)
    level("L", 2)
    begin("W1")
    pass_over(SLOTS_AT[0])
    need([1, 2, 3])
    attend(0, 4)
    pass_over(SLOTS_AT[1])
    level("L", 3)
    begin("W2")
    need([4, 5, 6, 7])
    attend(4, 4)
    level("W1", 1)
    level("L", 4)
    pass_over(SLOTS_AT[2])
    need([8, 9, 10, 11])
    attend(8, 4)
    pass_over(SLOTS_AT[3])
    need([12, 13, 14, 15])
    attend(12, 4)

    out_lat = (acc[...] / jnp.sum(l_run[...], axis=1, keepdims=True)).astype(BF16)
    vu_copy.wait()
    wide2[...] = value_up[...].astype(F32)
    squares = jnp.zeros((ROWS, 1), F32)
    gated = []
    for h in range(2):
        c = slice(h * VDIM, (h + 1) * VDIM)
        head_out = jnp.dot(
            out_lat[h * ROWS : (h + 1) * ROWS],
            wide2[pl.ds(h, LATENT, stride=2), :].astype(BF16),
            preferred_element_type=F32,
        )
        squares = squares + jnp.sum(head_out * head_out, axis=1, keepdims=True)
        gated.append((head_out * out_gain[:, c]).astype(BF16))
    gated = jnp.concatenate(gated, axis=1)

    def two_terms(total, rows):
        high = total.astype(BF16).astype(F32)
        at_lane = lax.broadcasted_iota(jnp.int32, (rows, 128), 1)
        return jnp.where(at_lane == 0, high, jnp.where(at_lane == 1, total - high, 0.0)).astype(BF16)

    ow_copy.wait()
    tail = two_terms(squares, ROWS)
    for c in range(0, D, 512):
        piece = jnp.dot(gated, out_w[:, c : c + 512], preferred_element_type=F32).astype(BF16)
        proj[:, :, :, c : c + 512] = piece.reshape(SIDE, 2, OWN, 512)
    proj[:, :, :, D:EXT] = tail.reshape(SIDE, 2, OWN, 128)

    swap = remote(proj.at[:, other], sib, ps.at[0], pr.at[0], sibling)
    swap.start()
    swap.wait_recv()
    sends = [swap]

    def chip_sum(k):
        who = (x + k) % SIDE
        both = proj[who, core].astype(F32) + sib[who].astype(F32)
        total = jnp.sum(both[:, D:EXT], axis=1, keepdims=True)
        return both[:, :D], total

    for k in (1, 3, 2):
        body, total = chip_sum(k)
        xs[k - 1, :, 0:D] = body.astype(BF16)
        xs[k - 1, :, D:EXT] = two_terms(total, OWN)
        c = remote(xs.at[k - 1], rx.at[k - 1], ps.at[k], pr.at[k], across(k))
        c.start()
        sends.append(c)
    projected, total = chip_sum(0)
    level("W1", 2)
    level("W2", 1)
    for k in (1, 3, 2):
        remote(rx.at[k - 1], rx.at[k - 1], ps.at[k], pr.at[k], across(k)).wait_recv()
        projected = projected + rx[k - 1, :, 0:D].astype(F32)
        total = total + jnp.sum(rx[k - 1, :, D:EXT].astype(F32), axis=1, keepdims=True)
    row_scale = lax.rsqrt(total / (HEADS * VDIM) + EPS)
    st_copy.wait()
    middle = stream[...].astype(F32) + row_scale * projected
    mid[...] = middle
    ff_row = (
        middle
        * lax.rsqrt(jnp.mean(middle * middle, axis=-1, keepdims=True) + EPS)
        * norm_gain[...]
    ).astype(BF16)
    fin[tp] = ff_row

    def row_copy(k, to, src_tp):
        v = fin.at[src_tp]
        return remote(v, v, fs.at[k], fr.at[k], to)

    for k in (1, 3, 2):
        c = row_copy(k, across(k), tp)
        c.start()
        sends.append(c)
    c = row_copy(0, sibling, tp)
    c.start()
    sends.append(c)
    level("W2", 2)
    level("W1", 3)
    for k in (1, 3, 2):
        came = ((x + SIDE - k) % SIDE) * 2
        row_copy(k, across(k), came + core).wait_recv()
        c = row_copy(3 + k, sibling, came + core)
        c.start()
        sends.append(c)
    row_copy(0, sibling, x * 2 + other).wait_recv()
    for k in (1, 3, 2):
        came = ((x + SIDE - k) % SIDE) * 2
        row_copy(3 + k, sibling, came + other).wait_recv()

    level("W2", 3)
    level("W1", 4)
    w1_copy.wait()
    w2_copy.wait()
    rows = fin[...].reshape(ROWS, D)
    for c in range(0, HID, 256):
        pre = jnp.dot(
            rows, w1[:, :, c : c + 256].reshape(D, 256), preferred_element_type=F32
        )
        act[:, c : c + 256] = jnp.square(jnp.maximum(pre, 0.0)).astype(BF16)

    def swap_part(g):
        return remote(part.at[g, :, other], psib.at[g], gs.at[g, 0], gr.at[g, 0], sibling)

    def x_part(g, k):
        return remote(pxs.at[g, k - 1], prx.at[g, k - 1], gs.at[g, k], gr.at[g, k], across(k))

    def ff_group(g):
        for n, f in enumerate(COLUMNS[4 * g : 4 * g + 4]):
            piece = jnp.dot(act[...], w2[block_at(*f)], preferred_element_type=F32).astype(BF16)
            part[g, :, :, :, n * 128 : (n + 1) * 128] = piece.reshape(SIDE, 2, OWN, 128)
        swap_part(g).start()

    def ff_chip(g):
        swap_part(g).wait_recv()
        for k in (1, 3, 2, 0):
            who = (x + k) % SIDE
            both = part[g, who, core].astype(F32) + psib[g, who].astype(F32)
            if k:
                pxs[g, k - 1] = both.astype(BF16)
                x_part(g, k).start()
            else:
                fsum[g] = both

    def ff_end(g):
        both = fsum[g]
        for k in (1, 3, 2):
            x_part(g, k).wait_recv()
            both = both + prx[g, k - 1].astype(F32)
        for n, f in enumerate(COLUMNS[4 * g : 4 * g + 4]):
            c = pl.ds(pl.multiple_of(block_at(*f) * 128, 128), 128)
            out[:, c] = (mid[:, c] + both[:, n * 128 : (n + 1) * 128]).astype(BF16)

    ff_group(0)
    ff_group(1)
    ff_chip(0)
    level("W2", 4)
    ff_group(2)
    ff_chip(1)
    ff_group(3)
    ff_chip(2)
    ff_end(0)
    ff_chip(3)
    ff_end(1)
    ff_end(2)
    ff_end(3)

    for g in ("L", "W1", "W2"):
        for m in MSGS:
            copy_of(g, m).wait_send()
    for slot in range(1, BLOCKS):
        along_x(slot).wait_send()
        share(slot).wait_send()
    for c in sends:
        c.wait_send()
    for g in range(4):
        swap_part(g).wait_send()
        for k in (1, 2, 3):
            x_part(g, k).wait_send()


def body(
    stream,
    query_nope,
    query_rope,
    latent,
    rope_key,
    latent_gain,
    key_up,
    value_up,
    out_gain,
    out_weight,
    norm_gain,
    ff_in,
    ff_out,
):
    near, far = rotary_tables()
    vmem = pl.BlockSpec(memory_space=pltpu.VMEM)
    hbm = pl.BlockSpec(memory_space=pl.ANY)
    dma = pltpu.SemaphoreType.DMA
    return pl.pallas_call(
        kernel,
        out_shape=jax.ShapeDtypeStruct((OWN, D), BF16),
        in_specs=[hbm, hbm, hbm, hbm, hbm, vmem, hbm, hbm, vmem, hbm, vmem, hbm, hbm, hbm, hbm],
        out_specs=vmem,
        scratch_shapes=[
            pltpu.VMEM((2 * ROWS, NOPE), BF16),
            pltpu.VMEM((2, ROPE, ROWS), BF16),
            pltpu.VMEM((ROWS, LATENT), BF16),
            pltpu.VMEM((ROPE, ROWS), BF16),
            pltpu.VMEM((2 * LATENT, NOPE), BF16),
            pltpu.VMEM((2 * LATENT, VDIM), BF16),
            pltpu.VMEM((ROPE, ROWS), F32),
            pltpu.VMEM((BLOCKS * PAIR, PACK), BF16),
            pltpu.VMEM((BLOCKS, D // BLOCKS, HID), BF16),
            pltpu.VMEM((BLOCKS, HID, D // BLOCKS), BF16),
            pltpu.VMEM((2 * ROWS, LATENT + 128), BF16),
            pltpu.VMEM((2 * ROWS, LATENT + 128), BF16),
            pltpu.VMEM((2 * ROWS, UNIT), F32),
            pltpu.VMEM((2 * ROWS, UNIT), F32),
            pltpu.VMEM((2 * ROWS, UNIT), BF16),
            pltpu.VMEM((2 * ROWS, UNIT), BF16),
            pltpu.VMEM((2 * ROWS, LATENT), F32),
            pltpu.VMEM((2 * ROWS, 128), F32),
            pltpu.VMEM((2 * ROWS, 128), F32),
            pltpu.VMEM((ROPE, 128), F32),
            pltpu.VMEM((OWN, D), BF16),
            pltpu.VMEM((2 * VDIM, D), BF16),
            pltpu.VMEM((SIDE, 2, OWN, EXT), BF16),
            pltpu.VMEM((SIDE, OWN, EXT), BF16),
            pltpu.VMEM((SIDE - 1, OWN, EXT), BF16),
            pltpu.VMEM((SIDE - 1, OWN, EXT), BF16),
            pltpu.VMEM((2 * SIDE, OWN, D), BF16),
            pltpu.VMEM((ROWS, HID), BF16),
            pltpu.VMEM((4, SIDE, 2, OWN, 512), BF16),
            pltpu.VMEM((4, SIDE, OWN, 512), BF16),
            pltpu.VMEM((4, SIDE - 1, OWN, 512), BF16),
            pltpu.VMEM((4, SIDE - 1, OWN, 512), BF16),
            pltpu.VMEM((OWN, D), F32),
            pltpu.VMEM((4, OWN, 512), F32),
            pltpu.VMEM((2 * ROWS, NOPE), F32),
            pltpu.VMEM((2 * LATENT, NOPE), F32),
            dma((BLOCKS,)),
            dma((BLOCKS,)),
            dma((12,)),
            dma((NMSG,)),
            dma((NMSG,)),
            dma((NMSG,)),
            dma((NMSG,)),
            dma((NMSG,)),
            dma((NMSG,)),
            dma((BLOCKS,)),
            dma((BLOCKS,)),
            dma((4,)),
            dma((4,)),
            dma((7,)),
            dma((7,)),
            dma((4, 4)),
            dma((4, 4)),
        ],
        compiler_params=pltpu.CompilerParams(
            collective_id=0, has_side_effects=True, vmem_limit_bytes=60 * 1024 * 1024
        ),
    )(
        stream,
        query_nope.reshape(2 * ROWS, NOPE),
        jnp.transpose(query_rope, (1, 2, 0)),
        latent,
        jnp.transpose(rope_key, (1, 0)),
        latent_gain.reshape(1, LATENT),
        key_up.reshape(2 * LATENT, NOPE),
        value_up.reshape(2 * LATENT, VDIM),
        out_gain.reshape(1, 2 * VDIM),
        out_weight,
        norm_gain.reshape(1, D),
        ff_in,
        ff_out,
        jnp.asarray(near),
        jnp.asarray(far),
    )


def solution(mesh):
    placed = (
        P(("sp", "tp"), None),
        P("sp", "tp", None),
        P("sp", "tp", None),
        P("sp", None),
        P("sp", None),
        P(),
        P(None, "tp", None),
        P(None, "tp", None),
        P("tp"),
        P("tp", None),
        P(),
        P("sp", "tp"),
        P("tp", "sp"),
    )
    return jax.shard_map(
        body, mesh=mesh, in_specs=placed, out_specs=P(("sp", "tp"), None), check_vma=False
    )
```

```python
import math

import jax
import jax.numpy as jnp
import numpy as np
from jax import lax
from jax.experimental import pallas as pl
from jax.experimental.pallas import tpu as pltpu
from jax.sharding import PartitionSpec as P

MESH = pl.DeviceIdType.MESH
F32 = jnp.float32
BF16 = jnp.bfloat16

HEADS = 16
NOPE = 128
ROPE = 64
LATENT = 512
VDIM = 128
EPS = 1e-06
THETA = 10000.0

SIDE = 4
BLOCKS = SIDE * SIDE
ROWS = 384
OWN = 48
D = 2048
HID = 1024
PACK = 1152
PAIR = ROWS // 2
EXT = D + 128
UNIT = 1024

UP, UM, VP, VM = (1, 0), (-1, 0), (0, 1), (0, -1)
LINKS = (UP, UM, VP, VM)


def wrap(v):
    return ((v[0] + 4) % 4, (v[1] + 4) % 4)


class Msg:
    def __init__(self, d, e, half, parent):
        self.d, self.e, self.half = d, wrap(e), half
        self.f = wrap((e[0] - d[0], e[1] - d[1]))
        self.level = 1 if parent is None else parent.level + 1
        self.kids = []
        self.id = None


def forwards(m):
    onward = m.d in ((UP, VP) if m.half == 0 else (UM, VM))
    if m.d[1] == 0:
        return ([m.d] if onward and m.f[0] != 2 else []) + [VP, VM]
    return [m.d] if onward and m.f[1] != 2 else []


def build_messages(half):
    todo = [Msg(d, (0, 0), half, None) for d in LINKS]
    done = []
    while todo:
        m = todo.pop(0)
        m.id = half * (BLOCKS - 1) + len(done)
        done.append(m)
        m.kids = [Msg(d, m.f, half, m) for d in forwards(m)]
        todo += m.kids
    return done


TREES = [build_messages(half) for half in (0, 1)]
assert all(sorted({m.f for m in t} | {(0, 0)}) == [(i, j) for i in range(4) for j in range(4)] for t in TREES)
NMSG = 2 * (BLOCKS - 1)
LEVELS = [[[m for m in t if m.level == k] for k in (1, 2, 3, 4)] for t in TREES]
ORDER = [(0, 0)] + [m.f for m in TREES[0]]
SLOT = {f: k for k, f in enumerate(ORDER)}

NEAR = 5
THIRD = PAIR // 6
DIRECT, OVER_X = {}, {}
SHARED = {k: 0 if k < 4 else 1 if k < 11 else 2 if k < 15 else 3 for k in range(1, 16)}
PASSED = {k: 0 if k < 11 else 1 if k < 15 else 2 for k in range(5, 16)}
_row = NEAR * PAIR
for _slots, _table, _rows in (
    (range(5, 11), DIRECT, 4 * THIRD),
    (range(11, 15), DIRECT, 4 * THIRD),
    (range(5, 11), OVER_X, 2 * THIRD),
    (range(15, 16), DIRECT, 4 * THIRD),
    (range(11, 15), OVER_X, 2 * THIRD),
    (range(15, 16), OVER_X, 2 * THIRD),
):
    for _slot in _slots:
        _table[_slot] = _row
        _row += _rows
assert _row == BLOCKS * PAIR

PARTS = ((0, 32), (32, 48))
EDGES = (0, 5, 11, 16)
GROUPS = len(EDGES) - 1


def rotary_tables():
    half = ROPE // 2
    inverse = np.power(THETA, -np.arange(0, ROPE, 2, dtype=np.float64) / ROPE)
    base = inverse[:, None] * np.arange(ROWS)[None, :]
    start = inverse[None, :] * (ROWS * np.arange(BLOCKS))[:, None]
    near = np.concatenate([np.cos(base), np.sin(base)], 0).astype(np.float32)
    far = np.concatenate([np.cos(start), np.sin(start)], 1).astype(np.float32)
    far = np.repeat(far[:, :, None], 128, axis=2)
    assert far.shape == (BLOCKS, 2 * half, 128)
    return near, far


def kernel(
    stream_in,
    qn_in,
    qr_in,
    latent_in,
    kr_in,
    lat_gain,
    key_up_in,
    value_up_in,
    out_gain,
    out_w_in,
    norm_gain,
    ff_in,
    ff_out,
    near_in,
    far_in,
    out,
    qn,
    qr_t,
    latent,
    kr_t,
    key_up,
    value_up,
    near,
    cat,
    w1,
    w2,
    qa,
    qb,
    sa,
    sb,
    pa,
    pb,
    acc,
    m_run,
    l_run,
    far,
    stream,
    out_w,
    proj,
    sib,
    xs,
    rx,
    fin,
    act,
    part,
    psib,
    pxs,
    prx,
    mid,
    fsum,
    sums,
    wide,
    wide2,
    er,
    xlr,
    xdr,
    loc_sem,
    ls,
    lr,
    s1,
    r1,
    s2,
    r2,
    dr,
    ps,
    pr,
    fr,
    gr,
):
    sp = lax.axis_index("sp")
    tp = lax.axis_index("tp")
    z, y = sp // SIDE, sp % SIDE
    x, core = tp // 2, tp % 2
    other = 1 - core


    def block_at(dy, dz):
        return ((z + dz) % SIDE) * SIDE + (y + dy) % SIDE

    def at(f):
        return block_at(f[0] * other + f[1] * core, f[0] * core + f[1] * other)

    def torus(d):
        return (at(wrap(d)), tp)

    sibling = (sp, x * 2 + other)

    def across(k):
        return (sp, ((x + k) % SIDE) * 2 + core)

    barrier = pltpu.get_barrier_semaphore()
    peers = [torus(d) for d in LINKS] + [sibling] + [across(k) for k in (1, 2, 3)]
    for peer in peers:
        pl.semaphore_signal(barrier, inc=1, device_id=peer, device_id_type=MESH)

    def local(src, dst, k):
        c = pltpu.make_async_copy(src, dst, loc_sem.at[k])
        c.start()
        return c

    early = [
        local(latent_in, latent, 5),
        local(far_in.at[sp], far, 0),
        local(near_in, near, 6),
        local(kr_in, kr_t, 7),
    ]
    early2 = [local(qn_in, qn, 8), local(key_up_in, key_up, 9), local(qr_in, qr_t, 10)]
    vu_copy = local(value_up_in, value_up, 11)
    w1_copy = local(ff_in, w1.at[sp], 1)
    w2_copy = local(ff_out, w2.at[sp], 2)
    ow_copy = local(out_w_in, out_w, 3)
    st_copy = local(stream_in, stream, 4)

    def remote(src, dst, ssem, rsem, dev):
        return pltpu.make_async_remote_copy(
            src_ref=src, dst_ref=dst, send_sem=ssem, recv_sem=rsem, device_id=dev, device_id_type=MESH
        )

    odd = x % 2

    def lat_rows(start, count):
        return cat.at[pl.ds(pl.multiple_of(start, 32), count), :]

    def lat_view(f, half):
        slot = SLOT[f]
        if slot < NEAR:
            return lat_rows(slot * PAIR + core * 3 * THIRD + (odd + half) * THIRD, THIRD)
        return lat_rows(DIRECT[slot] + core * 2 * THIRD + half * THIRD, THIRD)

    def rest_view(f):
        return lat_rows(SLOT[f] * PAIR + core * 3 * THIRD + (1 - odd) * 2 * THIRD, THIRD)

    def rest_copy(n):
        m = LEVELS[0][0][n]
        return remote(rest_view(m.e), rest_view(m.f), ls.at[0], er.at[0], torus(m.d))

    def in_view(f, half):
        return w1.at[at(f), pl.ds(half * 64, 64), :]

    def in_src(f, half):
        return ff_in.at[pl.ds(half * 64, 64), :] if f == (0, 0) else in_view(f, half)

    def out_view(f, half):
        return w2.at[at(f), pl.ds(half * 512, 512), :]

    def out_src(f, half):
        return ff_out.at[pl.ds(half * 512, 512), :] if f == (0, 0) else out_view(f, half)

    gathers = {
        "L": (lat_view, lat_view, ls, lr),
        "W1": (in_src, in_view, s1, r1),
        "W2": (out_src, out_view, s2, r2),
    }

    def copy_of(g, m):
        src, view, ssem, rsem = gathers[g]
        dst = view(m.f if g == "L" else m.e, m.half)
        k = m.id if g == "L" else m.half * 4 + m.level - 1
        return remote(src(m.e, m.half), dst, ssem.at[0], rsem.at[k], torus(m.d))

    def direct_rows(slot, who):
        if slot < NEAR:
            return lat_rows(slot * PAIR + who * 3 * THIRD, 3 * THIRD)
        return lat_rows(DIRECT[slot] + who * 2 * THIRD, 2 * THIRD)

    def x_rows(slot, who):
        return lat_rows(OVER_X[slot] + who * THIRD, THIRD)

    def share(slot):
        v = direct_rows(slot, core)
        return remote(v, v, ls.at[0], dr.at[SHARED[slot]], sibling)

    def share_x(slot):
        v = x_rows(slot, core)
        return remote(v, v, ls.at[0], xdr.at[PASSED[slot]], sibling)

    def along_x(slot):
        src = lat_rows(DIRECT[slot] + core * 2 * THIRD + odd * THIRD, THIRD)
        to = across(1 if slot % 2 == 0 else 3)
        return remote(src, x_rows(slot, core), ls.at[0], xlr.at[PASSED[slot]], to)

    def await_rows(count, sem):
        v = cat.at[pl.ds(0, count), :]
        remote(v, v, ls.at[0], sem, sibling).wait_recv()

    def pass_over(group):
        slots = [k for k in PASSED if PASSED[k] == group]
        await_rows(THIRD * len(slots), xlr.at[group])
        for slot in slots:
            share_x(slot).start()

    def need(direct, over):
        for group in direct:
            await_rows(
                sum((3 if k < NEAR else 2) * THIRD for k in SHARED if SHARED[k] == group), dr.at[group]
            )
        for group in over:
            await_rows(sum(THIRD for k in PASSED if PASSED[k] == group), xdr.at[group])

    def rest():
        await_rows(len(LINKS) * THIRD, er.at[0])
        for m in LEVELS[0][0]:
            share(SLOT[m.f]).start()

    def begin(g, half):
        for m in LEVELS[half][0]:
            copy_of(g, m).start()

    landed = {}

    def level(g, half, k):
        src, view, ssem, rsem = gathers[g]
        here = LEVELS[half][k - 1]
        if g != "L":
            whole = w1 if g == "W1" else w2
            tall = whole.shape[1] // 2
            if len(here) % 2:
                v = whole.at[0, pl.ds(0, tall), :]
            else:
                v = whole.at[pl.ds(0, len(here) // 2)]
            remote(v, v, ssem.at[0], rsem.at[half * 4 + k - 1], sibling).wait_recv()
        for m in here:
            if g == "L":
                v = view(m.f, half)
                remote(v, v, ssem.at[0], rsem.at[m.id], sibling).wait_recv()
            for kid in m.kids:
                copy_of(g, kid).start()
            if g == "L":
                landed[m.f] = landed.get(m.f, 0) + 1
                if landed[m.f] == 2 and k > 1:
                    along_x(SLOT[m.f]).start()
                    share(SLOT[m.f]).start()

    for c in early:
        c.wait()
    lat = latent[...].astype(F32)
    normed = (
        lat * lax.rsqrt(jnp.mean(lat * lat, axis=-1, keepdims=True) + EPS) * lat_gain[...]
    ).astype(BF16)
    cat[0:PAIR, 0:LATENT] = normed[:PAIR]
    cat[0:PAIR, LATENT + 128 : PACK] = normed[PAIR:]
    half = ROPE // 2
    cos_n, sin_n = near[0:half, :], near[half:ROPE, :]
    cos_f = jnp.broadcast_to(far[0:half, 0:1], (half, ROWS))
    sin_f = jnp.broadcast_to(far[half:ROPE, 0:1], (half, ROWS))
    cosine = cos_n * cos_f - sin_n * sin_f
    sine = sin_n * cos_f + cos_n * sin_f

    def turned(v):
        low, high = v[:half].astype(F32), v[half:].astype(F32)
        a = low * cosine - high * sine
        b = low * sine + high * cosine
        return jnp.transpose(jnp.concatenate([a, b, a, b], axis=0))

    lane = lax.broadcasted_iota(jnp.int32, (ROWS, 128), 1)
    keys = turned(kr_t[...])
    cat[0:PAIR, LATENT : LATENT + 128] = jnp.where(
        lane[:PAIR] < ROPE, keys[:PAIR], keys[PAIR:]
    ).astype(BF16)

    pl.semaphore_wait(barrier, len(peers))
    begin("L", 0)
    begin("L", 1)
    for n in range(len(LINKS)):
        rest_copy(n).start()

    for c in early2:
        c.wait()
    wide[0 : 2 * ROWS, :] = qn[...].astype(F32)
    wide2[...] = key_up[...].astype(F32)
    for h in range(2):
        rows = slice(h * ROWS, (h + 1) * ROWS)
        q_lat = lax.dot_general(
            wide[pl.ds(h, ROWS, stride=2), :].astype(BF16),
            wide2[pl.ds(h, LATENT, stride=2), :].astype(BF16),
            (((1,), (1,)), ((), ())),
            preferred_element_type=F32,
        ).astype(BF16)
        q_rot = turned(qr_t[h])
        qa[rows, 0:LATENT] = q_lat
        qa[rows, LATENT : LATENT + 128] = jnp.where(lane < ROPE, q_rot, 0.0).astype(BF16)
        qb[rows, 128 : LATENT + 128] = q_lat
        qb[rows, 0:128] = jnp.where(lane < ROPE, 0.0, q_rot).astype(BF16)

    acc[...] = jnp.zeros_like(acc)
    m_run[...] = jnp.full_like(m_run, -1e30)
    l_run[...] = jnp.zeros_like(l_run)
    factor = math.log2(math.e) / math.sqrt(NOPE + ROPE)

    def score(q, row, count, first):
        return lax.dot_general(
            q[...],
            cat[row : row + count, first : first + LATENT + 128],
            (((1,), (1,)), ((), ())),
            preferred_element_type=F32,
        )

    def weigh(s_ref, p_ref, row, count, first):
        scores = s_ref[:, 0:count]
        before = m_run[...]
        now = jnp.maximum(before, jnp.max(scores, axis=1, keepdims=True) * factor)
        fade = jnp.exp2(before - now)
        total = l_run[...] * fade
        for k in range(count // 128):
            expo = jnp.exp2(scores[:, k * 128 : (k + 1) * 128] * factor - now)
            total = total + expo
            p_ref[:, k * 128 : (k + 1) * 128] = expo.astype(BF16)
        l_run[...] = total
        m_run[...] = now
        mixed = jnp.dot(
            p_ref[:, 0:count],
            cat[row : row + count, first : first + LATENT],
            preferred_element_type=F32,
        )
        for k in range(LATENT // 128):
            c = slice(k * 128, (k + 1) * 128)
            acc[:, c] = acc[:, c] * fade + mixed[:, c]

    def attend(row, count, between=()):
        sa[:, 0:count] = score(qa, row, count, 0)
        sb[:, 0:count] = score(qb, row, count, LATENT)
        weigh(sa, pa, row, count, 0)
        for g, half, k in between:
            level(g, half, k)
        weigh(sb, pb, row, count, LATENT + 128)

    level("L", 0, 1)
    level("L", 1, 1)
    begin("W1", 0)
    rest()
    need([0], [])
    attend(0, 768)
    level("L", 0, 2)
    level("L", 1, 2)
    begin("W1", 1)
    need([1], [])
    attend(768, 768)
    level("L", 0, 3)
    level("L", 1, 3)
    level("W1", 0, 1)
    begin("W2", 0)
    pass_over(0)
    need([2], [0])
    attend(1536, 1024, [("L", 0, 4), ("L", 1, 4), ("W1", 1, 1)])
    begin("W2", 1)
    pass_over(1)
    pass_over(2)
    need([3], [1, 2])
    attend(2560, 512, [("W1", 0, 2)])

    out_lat = (acc[...] / jnp.sum(l_run[...], axis=1, keepdims=True)).astype(BF16)
    vu_copy.wait()
    wide2[...] = value_up[...].astype(F32)
    squares = jnp.zeros((ROWS, 1), F32)
    gated = []
    for h in range(2):
        c = slice(h * VDIM, (h + 1) * VDIM)
        head_out = jnp.dot(
            out_lat[h * ROWS : (h + 1) * ROWS],
            wide2[pl.ds(h, LATENT, stride=2), :].astype(BF16),
            preferred_element_type=F32,
        )
        squares = squares + jnp.sum(head_out * head_out, axis=1, keepdims=True)
        gated.append((head_out * out_gain[:, c]).astype(BF16))
    gated = jnp.concatenate(gated, axis=1)

    def two_terms(total, rows):
        high = total.astype(BF16).astype(F32)
        at_lane = lax.broadcasted_iota(jnp.int32, (rows, 128), 1)
        return jnp.where(at_lane == 0, high, jnp.where(at_lane == 1, total - high, 0.0)).astype(BF16)

    ow_copy.wait()
    tail = two_terms(squares, ROWS)
    for c in range(0, D, 512):
        piece = jnp.dot(gated, out_w[:, c : c + 512], preferred_element_type=F32).astype(BF16)
        proj[:, :, :, c : c + 512] = piece.reshape(SIDE, 2, OWN, 512)
    proj[:, :, :, D:EXT] = tail.reshape(SIDE, 2, OWN, 128)

    def rows_of(p):
        return pl.ds(PARTS[p][0], PARTS[p][1] - PARTS[p][0])

    def swap(p):
        r = rows_of(p)
        return remote(proj.at[:, other, r, :], sib.at[:, r, :], ps.at[0], pr.at[p, 0], sibling)

    def x_copy(p, k):
        r = rows_of(p)
        return remote(xs.at[k - 1, r, :], rx.at[k - 1, r, :], ps.at[1], pr.at[p, 1], across(k))

    def chip_send(p):
        first, last = PARTS[p]
        r = slice(first, last)
        swap(p).wait_recv()
        for k in (2, 1, 3, 0):
            who = (x + k) % SIDE
            both = proj[who, core, r, :].astype(F32) + sib[who, r, :].astype(F32)
            total = jnp.sum(both[:, D:EXT], axis=1, keepdims=True)
            if k:
                xs[k - 1, r, 0:D] = both[:, :D].astype(BF16)
                xs[k - 1, r, D:EXT] = two_terms(total, last - first)
                x_copy(p, k).start()
            else:
                mid[r, :] = both[:, :D]
                sums[r, :] = jnp.broadcast_to(total, (last - first, 128))

    def row_copy(p, k, to, src_tp):
        v = fin.at[src_tp, rows_of(p), :]
        return remote(v, v, ps.at[2], fr.at[p, k if 1 <= k <= 3 else 0], to)

    def came_from(k):
        return ((x + SIDE - k) % SIDE) * 2

    def mid_rows(p):
        r = slice(*PARTS[p])
        projected = mid[r, :]
        total = sums[r, 0:1]
        came = rx.at[:, rows_of(p), :]
        remote(came, came, ps.at[1], pr.at[p, 1], sibling).wait_recv()
        for k in (1, 3, 2):
            projected = projected + rx[k - 1, r, 0:D].astype(F32)
            total = total + jnp.sum(rx[k - 1, r, D:EXT].astype(F32), axis=1, keepdims=True)
        row_scale = lax.rsqrt(total / (HEADS * VDIM) + EPS)
        middle = stream[r, :].astype(F32) + row_scale * projected
        mid[r, :] = middle
        fin[tp, r, :] = (
            middle
            * lax.rsqrt(jnp.mean(middle * middle, axis=-1, keepdims=True) + EPS)
            * norm_gain[...]
        ).astype(BF16)
        for k in (2, 1, 3):
            row_copy(p, k, across(k), tp).start()
        row_copy(p, 0, sibling, tp).start()

    def spread(p):
        for k in (1, 3, 2):
            row_copy(p, k, across(k), came_from(k) + core).wait_recv()
            row_copy(p, 3 + k, sibling, came_from(k) + core).start()

    def spread_end(p):
        v = fin.at[pl.ds(0, SIDE), rows_of(p), :]
        remote(v, v, ps.at[2], fr.at[p, 0], sibling).wait_recv()

    def ff_in_half(p):
        first, last = PARTS[p]
        rows = fin[:, first:last, :].reshape(8 * (last - first), D)
        for c in range(0, HID, 256):
            pre = jnp.dot(
                rows, w1[:, :, c : c + 256].reshape(D, 256), preferred_element_type=F32
            )
            act[8 * first : 8 * last, c : c + 256] = jnp.square(jnp.maximum(pre, 0.0)).astype(BF16)

    def columns_of(g):
        return pl.ds(EDGES[g] * 128, (EDGES[g + 1] - EDGES[g]) * 128)

    def swap_part(g, p):
        r, c = rows_of(p), columns_of(g)
        return remote(
            part.at[:, other, r, c], psib.at[:, r, c], ps.at[3], gr.at[g, p, 0], sibling
        )

    def x_part(g, p, k):
        r, c = rows_of(p), columns_of(g)
        return remote(
            pxs.at[k - 1, r, c], prx.at[k - 1, r, c], ps.at[4], gr.at[g, p, 1], across(k)
        )

    def ff_group(g, p):
        first, last = PARTS[p]
        for n in range(EDGES[g], EDGES[g + 1]):
            f = ORDER[n]
            piece = jnp.dot(
                act[8 * first : 8 * last, :], w2[block_at(*f)], preferred_element_type=F32
            ).astype(BF16)
            part[:, :, first:last, n * 128 : (n + 1) * 128] = piece.reshape(
                SIDE, 2, last - first, 128
            )
        swap_part(g, p).start()

    def ff_chip(g, p):
        r, c = slice(*PARTS[p]), slice(EDGES[g] * 128, EDGES[g + 1] * 128)
        swap_part(g, p).wait_recv()
        for k in (2, 1, 3, 0):
            who = (x + k) % SIDE
            both = part[who, core, r, c].astype(F32) + psib[who, r, c].astype(F32)
            if k:
                pxs[k - 1, r, c] = both.astype(BF16)
                x_part(g, p, k).start()
            else:
                fsum[r, c] = both

    def ff_end(g, p):
        r = slice(*PARTS[p])
        came = prx.at[:, rows_of(p), columns_of(g)]
        remote(came, came, ps.at[4], gr.at[g, p, 1], sibling).wait_recv()
        for n in range(EDGES[g], EDGES[g + 1]):
            here = slice(n * 128, (n + 1) * 128)
            both = fsum[r, here]
            for k in (1, 3, 2):
                both = both + prx[k - 1, r, here].astype(F32)
            c = pl.ds(pl.multiple_of(block_at(*ORDER[n]) * 128, 128), 128)
            out[r, c] = (mid[r, c] + both).astype(BF16)

    def sent(v, sem):
        remote(v, v, sem, sem, sibling).wait_send()

    swap(0).start()
    swap(1).start()
    level("W1", 1, 2)
    level("W2", 0, 1)
    chip_send(0)
    chip_send(1)
    level("W2", 1, 1)
    st_copy.wait()
    w1_copy.wait()
    w2_copy.wait()
    level("W1", 0, 3)
    level("W1", 1, 3)
    mid_rows(0)
    level("W2", 0, 2)
    mid_rows(1)
    level("W2", 1, 2)
    level("W1", 0, 4)
    level("W1", 1, 4)
    spread(0)
    spread_end(0)
    ff_in_half(0)
    spread(1)
    level("W2", 0, 3)
    ff_group(0, 0)
    ff_group(1, 0)
    ff_chip(0, 0)
    level("W2", 1, 3)
    spread_end(1)
    ff_in_half(1)
    ff_chip(1, 0)
    ff_group(0, 1)
    level("W2", 0, 4)
    ff_group(1, 1)
    ff_chip(0, 1)
    level("W2", 1, 4)
    ff_group(2, 0)
    ff_chip(1, 1)
    ff_group(2, 1)
    ff_chip(2, 0)
    ff_end(0, 0)
    ff_chip(2, 1)
    ff_end(1, 0)
    ff_end(0, 1)
    ff_end(1, 1)
    ff_end(2, 0)
    ff_end(2, 1)

    tree_rows = 2 * (BLOCKS - 1) * THIRD + len(LINKS) * THIRD
    over_rows = 2 * len(PASSED) * THIRD
    shared_rows = sum((3 if k < NEAR else 2) * THIRD for k in SHARED)
    sent(cat.at[pl.ds(0, tree_rows + over_rows + shared_rows), :], ls.at[0])
    sent(w1.at[pl.ds(0, BLOCKS - 1)], s1.at[0])
    sent(w2.at[pl.ds(0, BLOCKS - 1)], s2.at[0])
    sent(sib, ps.at[0])
    sent(xs, ps.at[1])
    sent(fin.at[pl.ds(0, 2 * SIDE - 1)], ps.at[2])
    sent(psib, ps.at[3])
    sent(pxs, ps.at[4])


def body(
    stream,
    query_nope,
    query_rope,
    latent,
    rope_key,
    latent_gain,
    key_up,
    value_up,
    out_gain,
    out_weight,
    norm_gain,
    ff_in,
    ff_out,
):
    near, far = rotary_tables()
    vmem = pl.BlockSpec(memory_space=pltpu.VMEM)
    hbm = pl.BlockSpec(memory_space=pl.ANY)
    dma = pltpu.SemaphoreType.DMA
    return pl.pallas_call(
        kernel,
        out_shape=jax.ShapeDtypeStruct((OWN, D), BF16),
        in_specs=[hbm, hbm, hbm, hbm, hbm, vmem, hbm, hbm, vmem, hbm, vmem, hbm, hbm, hbm, hbm],
        out_specs=vmem,
        scratch_shapes=[
            pltpu.VMEM((2 * ROWS, NOPE), BF16),
            pltpu.VMEM((2, ROPE, ROWS), BF16),
            pltpu.VMEM((ROWS, LATENT), BF16),
            pltpu.VMEM((ROPE, ROWS), BF16),
            pltpu.VMEM((2 * LATENT, NOPE), BF16),
            pltpu.VMEM((2 * LATENT, VDIM), BF16),
            pltpu.VMEM((ROPE, ROWS), F32),
            pltpu.VMEM((BLOCKS * PAIR, PACK), BF16),
            pltpu.VMEM((BLOCKS, D // BLOCKS, HID), BF16),
            pltpu.VMEM((BLOCKS, HID, D // BLOCKS), BF16),
            pltpu.VMEM((2 * ROWS, LATENT + 128), BF16),
            pltpu.VMEM((2 * ROWS, LATENT + 128), BF16),
            pltpu.VMEM((2 * ROWS, UNIT), F32),
            pltpu.VMEM((2 * ROWS, UNIT), F32),
            pltpu.VMEM((2 * ROWS, UNIT), BF16),
            pltpu.VMEM((2 * ROWS, UNIT), BF16),
            pltpu.VMEM((2 * ROWS, LATENT), F32),
            pltpu.VMEM((2 * ROWS, 128), F32),
            pltpu.VMEM((2 * ROWS, 128), F32),
            pltpu.VMEM((ROPE, 128), F32),
            pltpu.VMEM((OWN, D), BF16),
            pltpu.VMEM((2 * VDIM, D), BF16),
            pltpu.VMEM((SIDE, 2, OWN, EXT), BF16),
            pltpu.VMEM((SIDE, OWN, EXT), BF16),
            pltpu.VMEM((SIDE - 1, OWN, EXT), BF16),
            pltpu.VMEM((SIDE - 1, OWN, EXT), BF16),
            pltpu.VMEM((2 * SIDE, OWN, D), BF16),
            pltpu.VMEM((ROWS, HID), BF16),
            pltpu.VMEM((SIDE, 2, OWN, D), BF16),
            pltpu.VMEM((SIDE, OWN, D), BF16),
            pltpu.VMEM((SIDE - 1, OWN, D), BF16),
            pltpu.VMEM((SIDE - 1, OWN, D), BF16),
            pltpu.VMEM((OWN, D), F32),
            pltpu.VMEM((OWN, D), F32),
            pltpu.VMEM((OWN, 128), F32),
            pltpu.VMEM((2 * ROWS, NOPE), F32),
            pltpu.VMEM((2 * LATENT, NOPE), F32),
            dma((1,)),
            dma((3,)),
            dma((3,)),
            dma((12,)),
            dma((1,)),
            dma((NMSG,)),
            dma((1,)),
            dma((8,)),
            dma((1,)),
            dma((8,)),
            dma((4,)),
            dma((5,)),
            dma((2, 2)),
            dma((2, 4)),
            dma((GROUPS, 2, 2)),
        ],
        compiler_params=pltpu.CompilerParams(
            collective_id=0, has_side_effects=True, vmem_limit_bytes=60 * 1024 * 1024
        ),
    )(
        stream,
        query_nope.reshape(2 * ROWS, NOPE),
        jnp.transpose(query_rope, (1, 2, 0)),
        latent,
        jnp.transpose(rope_key, (1, 0)),
        latent_gain.reshape(1, LATENT),
        key_up.reshape(2 * LATENT, NOPE),
        value_up.reshape(2 * LATENT, VDIM),
        out_gain.reshape(1, 2 * VDIM),
        out_weight,
        norm_gain.reshape(1, D),
        ff_in,
        ff_out,
        jnp.asarray(near),
        jnp.asarray(far),
    )


def solution(mesh):
    placed = (
        P(("sp", "tp"), None),
        P("sp", "tp", None),
        P("sp", "tp", None),
        P("sp", None),
        P("sp", None),
        P(),
        P(None, "tp", None),
        P(None, "tp", None),
        P("tp"),
        P("tp", None),
        P(),
        P("sp", "tp"),
        P("tp", "sp"),
    )
    return jax.shard_map(
        body, mesh=mesh, in_specs=placed, out_specs=P(("sp", "tp"), None), check_vma=False
    )
```

```python
import math

import jax
import jax.numpy as jnp
import numpy as np
from jax import lax
from jax.experimental import pallas as pl
from jax.experimental.pallas import tpu as pltpu
from jax.sharding import PartitionSpec as P

MESH = pl.DeviceIdType.MESH
F32 = jnp.float32
BF16 = jnp.bfloat16

HEADS = 16
NOPE = 128
ROPE = 64
LATENT = 512
VDIM = 128
EPS = 1e-06
THETA = 10000.0

SIDE = 4
BLOCKS = SIDE * SIDE
ROWS = 384
OWN = 48
D = 2048
HID = 1024
PACK = 1152
PAIR = ROWS // 2
EXT = D + 128
UNIT = 1024

UP, UM, VP, VM = (1, 0), (-1, 0), (0, 1), (0, -1)
LINKS = (UP, UM, VP, VM)


def wrap(v):
    return ((v[0] + 4) % 4, (v[1] + 4) % 4)


class Msg:
    def __init__(self, d, e, half, parent):
        self.d, self.e, self.half = d, wrap(e), half
        self.f = wrap((e[0] - d[0], e[1] - d[1]))
        self.level = 1 if parent is None else parent.level + 1
        self.kids = []
        self.id = None


def forwards(m):
    onward = m.d in ((UP, VP) if m.half == 0 else (UM, VM))
    if m.d[1] == 0:
        return ([m.d] if onward and m.f[0] != 2 else []) + [VP, VM]
    return [m.d] if onward and m.f[1] != 2 else []


def build_messages(half):
    todo = [Msg(d, (0, 0), half, None) for d in LINKS]
    done = []
    while todo:
        m = todo.pop(0)
        m.id = half * (BLOCKS - 1) + len(done)
        done.append(m)
        m.kids = [Msg(d, m.f, half, m) for d in forwards(m)]
        todo += m.kids
    return done


TREES = [build_messages(half) for half in (0, 1)]
assert all(sorted({m.f for m in t} | {(0, 0)}) == [(i, j) for i in range(4) for j in range(4)] for t in TREES)
NMSG = 2 * (BLOCKS - 1)
LEVELS = [[[m for m in t if m.level == k] for k in (1, 2, 3, 4)] for t in TREES]
ORDER = [(0, 0)] + [m.f for m in TREES[0]]
SLOT = {f: k for k, f in enumerate(ORDER)}

NEAR = 5
THIRD = PAIR // 6
DIRECT, OVER_X = {}, {}
SHARED = {k: 0 if k < 4 else 1 if k < 11 else 2 if k < 15 else 3 for k in range(1, 16)}
PASSED = {k: 0 if k < 11 else 1 if k < 15 else 2 for k in range(5, 16)}
_row = NEAR * PAIR
for _slots, _table, _rows in (
    (range(5, 11), DIRECT, 4 * THIRD),
    (range(11, 15), DIRECT, 4 * THIRD),
    (range(5, 11), OVER_X, 2 * THIRD),
    (range(15, 16), DIRECT, 4 * THIRD),
    (range(11, 15), OVER_X, 2 * THIRD),
    (range(15, 16), OVER_X, 2 * THIRD),
):
    for _slot in _slots:
        _table[_slot] = _row
        _row += _rows
assert _row == BLOCKS * PAIR

PARTS = ((0, 16), (16, 32), (32, 48))
EDGES = (0, 5, 11, 15, 16)
GROUPS = len(EDGES) - 1


def rotary_tables():
    half = ROPE // 2
    inverse = np.power(THETA, -np.arange(0, ROPE, 2, dtype=np.float64) / ROPE)
    base = inverse[:, None] * np.arange(ROWS)[None, :]
    start = inverse[None, :] * (ROWS * np.arange(BLOCKS))[:, None]
    near = np.concatenate([np.cos(base), np.sin(base)], 0).astype(np.float32)
    far = np.concatenate([np.cos(start), np.sin(start)], 1).astype(np.float32)
    far = np.repeat(far[:, :, None], 128, axis=2)
    assert far.shape == (BLOCKS, 2 * half, 128)
    return near, far


def kernel(
    stream_in,
    qn_in,
    qr_in,
    latent_in,
    kr_in,
    lat_gain_in,
    key_up_in,
    value_up_in,
    out_gain_in,
    out_w_in,
    norm_gain_in,
    ff_in,
    ff_out,
    near_in,
    far_in,
    out,
    lat_gain,
    out_gain,
    norm_gain,
    qn,
    qr_t,
    latent,
    kr_t,
    key_up,
    value_up,
    near,
    cat,
    w1,
    w2,
    qa,
    qb,
    sa,
    sb,
    pa,
    pb,
    acc,
    m_run,
    l_run,
    far,
    stream,
    out_w,
    proj,
    sib,
    xs,
    rx,
    fin,
    act,
    part,
    psib,
    pxs,
    prx,
    mid,
    fsum,
    sums,
    wide,
    wide2,
    er,
    xlr,
    xdr,
    loc_sem,
    ls,
    lr,
    s1,
    r1,
    s2,
    r2,
    dr,
    ps,
    pr,
    fr,
    gr,
):
    sp = lax.axis_index("sp")
    tp = lax.axis_index("tp")
    z, y = sp // SIDE, sp % SIDE
    x, core = tp // 2, tp % 2
    other = 1 - core


    def block_at(dy, dz):
        return ((z + dz) % SIDE) * SIDE + (y + dy) % SIDE

    def at(f):
        return block_at(f[0] * other + f[1] * core, f[0] * core + f[1] * other)

    def torus(d):
        return (at(wrap(d)), tp)

    sibling = (sp, x * 2 + other)

    def across(k):
        return (sp, ((x + k) % SIDE) * 2 + core)

    barrier = pltpu.get_barrier_semaphore()
    peers = [torus(d) for d in LINKS] + [sibling] + [across(k) for k in (1, 2, 3)]
    for peer in peers:
        pl.semaphore_signal(barrier, inc=1, device_id=peer, device_id_type=MESH)

    def local(src, dst, k):
        c = pltpu.make_async_copy(src, dst, loc_sem.at[k])
        c.start()
        return c

    early = [
        local(latent_in, latent, 5),
        local(far_in.at[sp], far, 0),
        local(near_in, near, 6),
        local(kr_in, kr_t, 7),
        local(lat_gain_in, lat_gain, 12),
    ]
    og_copy = local(out_gain_in, out_gain, 13)
    ng_copy = local(norm_gain_in, norm_gain, 14)
    early2 = [local(qn_in, qn, 8), local(key_up_in, key_up, 9), local(qr_in, qr_t, 10)]
    vu_copy = local(value_up_in, value_up, 11)
    w1_copy = local(ff_in, w1.at[sp], 1)
    w2_copy = local(ff_out, w2.at[sp], 2)
    ow_copy = local(out_w_in, out_w, 3)
    st_copy = local(stream_in, stream, 4)

    def remote(src, dst, ssem, rsem, dev):
        return pltpu.make_async_remote_copy(
            src_ref=src, dst_ref=dst, send_sem=ssem, recv_sem=rsem, device_id=dev, device_id_type=MESH
        )

    odd = x % 2

    def lat_rows(start, count):
        return cat.at[pl.ds(pl.multiple_of(start, 32), count), :]

    def lat_view(f, half):
        slot = SLOT[f]
        if slot < NEAR:
            return lat_rows(slot * PAIR + core * 3 * THIRD + (odd + half) * THIRD, THIRD)
        return lat_rows(DIRECT[slot] + core * 2 * THIRD + half * THIRD, THIRD)

    def rest_view(f):
        return lat_rows(SLOT[f] * PAIR + core * 3 * THIRD + (1 - odd) * 2 * THIRD, THIRD)

    def rest_copy(n):
        m = LEVELS[0][0][n]
        return remote(rest_view(m.e), rest_view(m.f), ls.at[0], er.at[0], torus(m.d))

    def in_view(f, half):
        return w1.at[at(f), pl.ds(half * 64, 64), :]

    def in_src(f, half):
        return ff_in.at[pl.ds(half * 64, 64), :] if f == (0, 0) else in_view(f, half)

    def out_view(f, half):
        return w2.at[at(f), pl.ds(half * 512, 512), :]

    def out_src(f, half):
        return ff_out.at[pl.ds(half * 512, 512), :] if f == (0, 0) else out_view(f, half)

    gathers = {
        "L": (lat_view, lat_view, ls, lr),
        "W1": (in_src, in_view, s1, r1),
        "W2": (out_src, out_view, s2, r2),
    }

    def copy_of(g, m):
        src, view, ssem, rsem = gathers[g]
        dst = view(m.f if g == "L" else m.e, m.half)
        k = m.id if g == "L" else m.half * 4 + m.level - 1
        return remote(src(m.e, m.half), dst, ssem.at[0], rsem.at[k], torus(m.d))

    def direct_rows(slot, who):
        if slot < NEAR:
            return lat_rows(slot * PAIR + who * 3 * THIRD, 3 * THIRD)
        return lat_rows(DIRECT[slot] + who * 2 * THIRD, 2 * THIRD)

    def x_rows(slot, who):
        return lat_rows(OVER_X[slot] + who * THIRD, THIRD)

    def share(slot):
        v = direct_rows(slot, core)
        return remote(v, v, ls.at[0], dr.at[SHARED[slot]], sibling)

    def share_x(slot):
        v = x_rows(slot, core)
        return remote(v, v, ls.at[0], xdr.at[PASSED[slot]], sibling)

    def along_x(slot):
        src = lat_rows(DIRECT[slot] + core * 2 * THIRD + odd * THIRD, THIRD)
        to = across(1 if slot % 2 == 0 else 3)
        return remote(src, x_rows(slot, core), ls.at[0], xlr.at[PASSED[slot]], to)

    def await_rows(count, sem):
        v = cat.at[pl.ds(0, count), :]
        remote(v, v, ls.at[0], sem, sibling).wait_recv()

    def pass_over(group):
        slots = [k for k in PASSED if PASSED[k] == group]
        await_rows(THIRD * len(slots), xlr.at[group])
        for slot in slots:
            share_x(slot).start()

    def need(direct, over):
        for group in direct:
            await_rows(
                sum((3 if k < NEAR else 2) * THIRD for k in SHARED if SHARED[k] == group), dr.at[group]
            )
        for group in over:
            await_rows(sum(THIRD for k in PASSED if PASSED[k] == group), xdr.at[group])

    def rest():
        await_rows(len(LINKS) * THIRD, er.at[0])
        for m in LEVELS[0][0]:
            share(SLOT[m.f]).start()

    def begin(g, half):
        for m in LEVELS[half][0]:
            copy_of(g, m).start()

    landed = {}

    def level(g, half, k):
        src, view, ssem, rsem = gathers[g]
        here = LEVELS[half][k - 1]
        if g != "L":
            whole = w1 if g == "W1" else w2
            tall = whole.shape[1] // 2
            if len(here) % 2:
                v = whole.at[0, pl.ds(0, tall), :]
            else:
                v = whole.at[pl.ds(0, len(here) // 2)]
            remote(v, v, ssem.at[0], rsem.at[half * 4 + k - 1], sibling).wait_recv()
        for m in here:
            if g == "L":
                v = view(m.f, half)
                remote(v, v, ssem.at[0], rsem.at[m.id], sibling).wait_recv()
            for kid in m.kids:
                copy_of(g, kid).start()
            if g == "L":
                landed[m.f] = landed.get(m.f, 0) + 1
                if landed[m.f] == 2 and k > 1:
                    along_x(SLOT[m.f]).start()
                    share(SLOT[m.f]).start()

    for c in early:
        c.wait()
    lat = latent[...].astype(F32)
    normed = (
        lat * lax.rsqrt(jnp.mean(lat * lat, axis=-1, keepdims=True) + EPS) * lat_gain[...]
    ).astype(BF16)
    cat[0:PAIR, 0:LATENT] = normed[:PAIR]
    cat[0:PAIR, LATENT + 128 : PACK] = normed[PAIR:]
    half = ROPE // 2
    cos_n, sin_n = near[0:half, :], near[half:ROPE, :]
    cos_f = jnp.broadcast_to(far[0:half, 0:1], (half, ROWS))
    sin_f = jnp.broadcast_to(far[half:ROPE, 0:1], (half, ROWS))
    cosine = cos_n * cos_f - sin_n * sin_f
    sine = sin_n * cos_f + cos_n * sin_f

    def turned(v):
        low, high = v[:half].astype(F32), v[half:].astype(F32)
        a = low * cosine - high * sine
        b = low * sine + high * cosine
        return jnp.transpose(jnp.concatenate([a, b, a, b], axis=0))

    lane = lax.broadcasted_iota(jnp.int32, (ROWS, 128), 1)
    keys = turned(kr_t[...])
    cat[0:PAIR, LATENT : LATENT + 128] = jnp.where(
        lane[:PAIR] < ROPE, keys[:PAIR], keys[PAIR:]
    ).astype(BF16)

    pl.semaphore_wait(barrier, len(peers))
    begin("L", 0)
    begin("L", 1)
    for n in range(len(LINKS)):
        rest_copy(n).start()

    for c in early2:
        c.wait()
    wide[0 : 2 * ROWS, :] = qn[...].astype(F32)
    wide2[...] = key_up[...].astype(F32)
    for h in range(2):
        rows = slice(h * ROWS, (h + 1) * ROWS)
        q_lat = lax.dot_general(
            wide[pl.ds(h, ROWS, stride=2), :].astype(BF16),
            wide2[pl.ds(h, LATENT, stride=2), :].astype(BF16),
            (((1,), (1,)), ((), ())),
            preferred_element_type=F32,
        ).astype(BF16)
        q_rot = turned(qr_t[h])
        qa[rows, 0:LATENT] = q_lat
        qa[rows, LATENT : LATENT + 128] = jnp.where(lane < ROPE, q_rot, 0.0).astype(BF16)
        qb[rows, 128 : LATENT + 128] = q_lat
        qb[rows, 0:128] = jnp.where(lane < ROPE, 0.0, q_rot).astype(BF16)

    acc[...] = jnp.zeros_like(acc)
    m_run[...] = jnp.full_like(m_run, -1e30)
    l_run[...] = jnp.zeros_like(l_run)
    factor = math.log2(math.e) / math.sqrt(NOPE + ROPE)

    def score(q, row, count, first):
        return lax.dot_general(
            q[...],
            cat[row : row + count, first : first + LATENT + 128],
            (((1,), (1,)), ((), ())),
            preferred_element_type=F32,
        )

    def weigh(s_ref, p_ref, row, count, first):
        scores = s_ref[:, 0:count]
        before = m_run[...]
        now = jnp.maximum(before, jnp.max(scores, axis=1, keepdims=True) * factor)
        fade = jnp.exp2(before - now)
        total = l_run[...] * fade
        for k in range(count // 128):
            expo = jnp.exp2(scores[:, k * 128 : (k + 1) * 128] * factor - now)
            total = total + expo
            p_ref[:, k * 128 : (k + 1) * 128] = expo.astype(BF16)
        l_run[...] = total
        m_run[...] = now
        mixed = jnp.dot(
            p_ref[:, 0:count],
            cat[row : row + count, first : first + LATENT],
            preferred_element_type=F32,
        )
        for k in range(LATENT // 128):
            c = slice(k * 128, (k + 1) * 128)
            acc[:, c] = acc[:, c] * fade + mixed[:, c]

    def attend(row, count, between=None):
        sa[:, 0:count] = score(qa, row, count, 0)
        sb[:, 0:count] = score(qb, row, count, LATENT)
        weigh(sa, pa, row, count, 0)
        if between is not None:
            between()
        weigh(sb, pb, row, count, LATENT + 128)

    def last_latents():
        level("L", 0, 4)
        level("L", 1, 4)
        level("W1", 1, 1)

    level("L", 0, 1)
    level("L", 1, 1)
    rest()
    need([0], [])
    attend(0, 768, lambda: begin("W1", 0))
    level("L", 0, 2)
    level("L", 1, 2)
    need([1], [])
    attend(768, 768, lambda: begin("W1", 1))
    level("L", 0, 3)
    level("L", 1, 3)
    level("W1", 0, 1)
    begin("W2", 0)
    pass_over(0)
    need([2], [0])
    attend(1536, 1024, last_latents)
    begin("W2", 1)
    pass_over(1)
    pass_over(2)
    need([3], [1, 2])
    attend(2560, 512, lambda: level("W1", 0, 2))

    out_lat = (acc[...] / jnp.sum(l_run[...], axis=1, keepdims=True)).astype(BF16)
    vu_copy.wait()
    og_copy.wait()
    wide2[...] = value_up[...].astype(F32)
    squares = jnp.zeros((ROWS, 1), F32)
    gated = []
    for h in range(2):
        c = slice(h * VDIM, (h + 1) * VDIM)
        head_out = jnp.dot(
            out_lat[h * ROWS : (h + 1) * ROWS],
            wide2[pl.ds(h, LATENT, stride=2), :].astype(BF16),
            preferred_element_type=F32,
        )
        squares = squares + jnp.sum(head_out * head_out, axis=1, keepdims=True)
        gated.append((head_out * out_gain[:, c]).astype(BF16))
    gated = jnp.concatenate(gated, axis=1)

    def two_terms(total, rows):
        high = total.astype(BF16).astype(F32)
        at_lane = lax.broadcasted_iota(jnp.int32, (rows, 128), 1)
        return jnp.where(at_lane == 0, high, jnp.where(at_lane == 1, total - high, 0.0)).astype(BF16)

    ow_copy.wait()
    tail = two_terms(squares, ROWS)
    for c in range(0, D, 512):
        piece = jnp.dot(gated, out_w[:, c : c + 512], preferred_element_type=F32).astype(BF16)
        proj[:, :, :, c : c + 512] = piece.reshape(SIDE, 2, OWN, 512)
    proj[:, :, :, D:EXT] = tail.reshape(SIDE, 2, OWN, 128)

    def rows_of(p):
        return pl.ds(PARTS[p][0], PARTS[p][1] - PARTS[p][0])

    def swap(p):
        r = rows_of(p)
        return remote(proj.at[:, other, r, :], sib.at[:, r, :], ps.at[0], pr.at[p, 0], sibling)

    def x_copy(p, k):
        r = rows_of(p)
        return remote(xs.at[k - 1, r, :], rx.at[k - 1, r, :], ps.at[1], pr.at[p, 1], across(k))

    def chip_send(p):
        first, last = PARTS[p]
        r = slice(first, last)
        swap(p).wait_recv()
        for k in (2, 1, 3, 0):
            who = (x + k) % SIDE
            both = proj[who, core, r, :].astype(F32) + sib[who, r, :].astype(F32)
            total = jnp.sum(both[:, D:EXT], axis=1, keepdims=True)
            if k:
                xs[k - 1, r, 0:D] = both[:, :D].astype(BF16)
                xs[k - 1, r, D:EXT] = two_terms(total, last - first)
                x_copy(p, k).start()
            else:
                mid[r, :] = both[:, :D]
                sums[r, :] = jnp.broadcast_to(total, (last - first, 128))

    def row_copy(p, k, to, src_tp):
        v = fin.at[src_tp, rows_of(p), :]
        return remote(v, v, ps.at[2], fr.at[p, k if 1 <= k <= 3 else 0], to)

    def came_from(k):
        return ((x + SIDE - k) % SIDE) * 2

    def mid_rows(p):
        r = slice(*PARTS[p])
        projected = mid[r, :]
        total = sums[r, 0:1]
        came = rx.at[:, rows_of(p), :]
        remote(came, came, ps.at[1], pr.at[p, 1], sibling).wait_recv()
        for k in (1, 3, 2):
            projected = projected + rx[k - 1, r, 0:D].astype(F32)
            total = total + jnp.sum(rx[k - 1, r, D:EXT].astype(F32), axis=1, keepdims=True)
        row_scale = lax.rsqrt(total / (HEADS * VDIM) + EPS)
        middle = stream[r, :].astype(F32) + row_scale * projected
        mid[r, :] = middle
        fin[tp, r, :] = (
            middle
            * lax.rsqrt(jnp.mean(middle * middle, axis=-1, keepdims=True) + EPS)
            * norm_gain[...]
        ).astype(BF16)
        for k in (2, 1, 3):
            row_copy(p, k, across(k), tp).start()
        row_copy(p, 0, sibling, tp).start()

    def spread(p):
        for k in (1, 3, 2):
            row_copy(p, k, across(k), came_from(k) + core).wait_recv()
            row_copy(p, 3 + k, sibling, came_from(k) + core).start()

    def spread_end(p):
        v = fin.at[pl.ds(0, SIDE), rows_of(p), :]
        remote(v, v, ps.at[2], fr.at[p, 0], sibling).wait_recv()

    def ff_in_half(p):
        first, last = PARTS[p]
        rows = fin[:, first:last, :].reshape(8 * (last - first), D)
        for c in range(0, HID, 256):
            pre = jnp.dot(
                rows, w1[:, :, c : c + 256].reshape(D, 256), preferred_element_type=F32
            )
            act[8 * first : 8 * last, c : c + 256] = jnp.square(jnp.maximum(pre, 0.0)).astype(BF16)

    def columns_of(g):
        return pl.ds(EDGES[g] * 128, (EDGES[g + 1] - EDGES[g]) * 128)

    def swap_part(g, p):
        r, c = rows_of(p), columns_of(g)
        return remote(
            part.at[:, other, r, c], psib.at[:, r, c], ps.at[3], gr.at[g, p, 0], sibling
        )

    def x_part(g, p, k):
        r, c = rows_of(p), columns_of(g)
        return remote(
            pxs.at[k - 1, r, c], prx.at[k - 1, r, c], ps.at[4], gr.at[g, p, 1], across(k)
        )

    def ff_group(g, p):
        first, last = PARTS[p]
        for n in range(EDGES[g], EDGES[g + 1]):
            f = ORDER[n]
            piece = jnp.dot(
                act[8 * first : 8 * last, :], w2[block_at(*f)], preferred_element_type=F32
            ).astype(BF16)
            part[:, :, first:last, n * 128 : (n + 1) * 128] = piece.reshape(
                SIDE, 2, last - first, 128
            )
        swap_part(g, p).start()

    def ff_chip(g, p):
        r, c = slice(*PARTS[p]), slice(EDGES[g] * 128, EDGES[g + 1] * 128)
        swap_part(g, p).wait_recv()
        for k in (2, 1, 3, 0):
            who = (x + k) % SIDE
            both = part[who, core, r, c].astype(F32) + psib[who, r, c].astype(F32)
            if k:
                pxs[k - 1, r, c] = both.astype(BF16)
                x_part(g, p, k).start()
            else:
                fsum[r, c] = both

    def ff_end(g, p):
        r = slice(*PARTS[p])
        came = prx.at[:, rows_of(p), columns_of(g)]
        remote(came, came, ps.at[4], gr.at[g, p, 1], sibling).wait_recv()
        for n in range(EDGES[g], EDGES[g + 1]):
            here = slice(n * 128, (n + 1) * 128)
            both = fsum[r, here]
            for k in (1, 3, 2):
                both = both + prx[k - 1, r, here].astype(F32)
            c = pl.ds(pl.multiple_of(block_at(*ORDER[n]) * 128, 128), 128)
            out[r, c] = (mid[r, c] + both).astype(BF16)

    def sent(v, sem):
        remote(v, v, sem, sem, sibling).wait_send()

    for p in range(len(PARTS)):
        swap(p).start()
    level("W1", 1, 2)
    chip_send(0)
    chip_send(1)
    chip_send(2)
    level("W2", 0, 1)
    st_copy.wait()
    w1_copy.wait()
    w2_copy.wait()
    ng_copy.wait()
    level("W1", 0, 3)
    level("W2", 1, 1)
    mid_rows(0)
    level("W1", 1, 3)
    mid_rows(1)
    mid_rows(2)
    level("W2", 0, 2)
    spread(0)
    level("W2", 1, 2)
    level("W1", 0, 4)
    level("W1", 1, 4)
    spread_end(0)
    ff_in_half(0)
    ff_group(0, 0)
    spread(1)
    ff_group(1, 0)
    ff_chip(0, 0)
    spread_end(1)
    ff_in_half(1)
    ff_chip(1, 0)
    ff_group(0, 1)
    level("W2", 0, 3)
    spread(2)
    ff_group(1, 1)
    ff_chip(0, 1)
    spread_end(2)
    ff_in_half(2)
    ff_chip(1, 1)
    ff_group(0, 2)
    level("W2", 1, 3)
    ff_group(1, 2)
    ff_chip(0, 2)
    level("W2", 0, 4)
    ff_group(2, 0)
    ff_chip(1, 2)
    ff_group(2, 1)
    ff_chip(2, 0)
    ff_group(2, 2)
    ff_chip(2, 1)
    level("W2", 1, 4)
    ff_group(3, 0)
    ff_chip(2, 2)
    ff_group(3, 1)
    ff_group(3, 2)
    ff_end(0, 0)
    ff_end(0, 1)
    ff_chip(3, 0)
    ff_chip(3, 1)
    ff_chip(3, 2)
    ff_end(1, 0)
    ff_end(1, 1)
    ff_end(0, 2)
    ff_end(1, 2)
    ff_end(2, 0)
    ff_end(2, 1)
    ff_end(2, 2)
    ff_end(3, 0)
    ff_end(3, 1)
    ff_end(3, 2)

    tree_rows = 2 * (BLOCKS - 1) * THIRD + len(LINKS) * THIRD
    over_rows = 2 * len(PASSED) * THIRD
    shared_rows = sum((3 if k < NEAR else 2) * THIRD for k in SHARED)
    sent(cat.at[pl.ds(0, tree_rows + over_rows + shared_rows), :], ls.at[0])
    sent(w1.at[pl.ds(0, BLOCKS - 1)], s1.at[0])
    sent(w2.at[pl.ds(0, BLOCKS - 1)], s2.at[0])
    sent(sib, ps.at[0])
    sent(xs, ps.at[1])
    sent(fin.at[pl.ds(0, 2 * SIDE - 1)], ps.at[2])
    sent(psib, ps.at[3])
    sent(pxs, ps.at[4])


def body(
    stream,
    query_nope,
    query_rope,
    latent,
    rope_key,
    latent_gain,
    key_up,
    value_up,
    out_gain,
    out_weight,
    norm_gain,
    ff_in,
    ff_out,
):
    near, far = rotary_tables()
    vmem = pl.BlockSpec(memory_space=pltpu.VMEM)
    hbm = pl.BlockSpec(memory_space=pl.ANY)
    dma = pltpu.SemaphoreType.DMA
    return pl.pallas_call(
        kernel,
        out_shape=jax.ShapeDtypeStruct((OWN, D), BF16),
        in_specs=[hbm] * 15,
        out_specs=vmem,
        scratch_shapes=[
            pltpu.VMEM((1, LATENT), F32),
            pltpu.VMEM((1, 2 * VDIM), F32),
            pltpu.VMEM((1, D), F32),
            pltpu.VMEM((2 * ROWS, NOPE), BF16),
            pltpu.VMEM((2, ROPE, ROWS), BF16),
            pltpu.VMEM((ROWS, LATENT), BF16),
            pltpu.VMEM((ROPE, ROWS), BF16),
            pltpu.VMEM((2 * LATENT, NOPE), BF16),
            pltpu.VMEM((2 * LATENT, VDIM), BF16),
            pltpu.VMEM((ROPE, ROWS), F32),
            pltpu.VMEM((BLOCKS * PAIR, PACK), BF16),
            pltpu.VMEM((BLOCKS, D // BLOCKS, HID), BF16),
            pltpu.VMEM((BLOCKS, HID, D // BLOCKS), BF16),
            pltpu.VMEM((2 * ROWS, LATENT + 128), BF16),
            pltpu.VMEM((2 * ROWS, LATENT + 128), BF16),
            pltpu.VMEM((2 * ROWS, UNIT), F32),
            pltpu.VMEM((2 * ROWS, UNIT), F32),
            pltpu.VMEM((2 * ROWS, UNIT), BF16),
            pltpu.VMEM((2 * ROWS, UNIT), BF16),
            pltpu.VMEM((2 * ROWS, LATENT), F32),
            pltpu.VMEM((2 * ROWS, 128), F32),
            pltpu.VMEM((2 * ROWS, 128), F32),
            pltpu.VMEM((ROPE, 128), F32),
            pltpu.VMEM((OWN, D), BF16),
            pltpu.VMEM((2 * VDIM, D), BF16),
            pltpu.VMEM((SIDE, 2, OWN, EXT), BF16),
            pltpu.VMEM((SIDE, OWN, EXT), BF16),
            pltpu.VMEM((SIDE - 1, OWN, EXT), BF16),
            pltpu.VMEM((SIDE - 1, OWN, EXT), BF16),
            pltpu.VMEM((2 * SIDE, OWN, D), BF16),
            pltpu.VMEM((ROWS, HID), BF16),
            pltpu.VMEM((SIDE, 2, OWN, D), BF16),
            pltpu.VMEM((SIDE, OWN, D), BF16),
            pltpu.VMEM((SIDE - 1, OWN, D), BF16),
            pltpu.VMEM((SIDE - 1, OWN, D), BF16),
            pltpu.VMEM((OWN, D), F32),
            pltpu.VMEM((OWN, D), F32),
            pltpu.VMEM((OWN, 128), F32),
            pltpu.VMEM((2 * ROWS, NOPE), F32),
            pltpu.VMEM((2 * LATENT, NOPE), F32),
            dma((1,)),
            dma((3,)),
            dma((3,)),
            dma((15,)),
            dma((1,)),
            dma((NMSG,)),
            dma((1,)),
            dma((8,)),
            dma((1,)),
            dma((8,)),
            dma((4,)),
            dma((5,)),
            dma((3, 2)),
            dma((3, 4)),
            dma((GROUPS, 3, 2)),
        ],
        compiler_params=pltpu.CompilerParams(
            collective_id=0, has_side_effects=True, vmem_limit_bytes=60 * 1024 * 1024
        ),
    )(
        stream,
        query_nope.reshape(2 * ROWS, NOPE),
        jnp.transpose(query_rope, (1, 2, 0)),
        latent,
        jnp.transpose(rope_key, (1, 0)),
        latent_gain.reshape(1, LATENT),
        key_up.reshape(2 * LATENT, NOPE),
        value_up.reshape(2 * LATENT, VDIM),
        out_gain.reshape(1, 2 * VDIM),
        out_weight,
        norm_gain.reshape(1, D),
        ff_in,
        ff_out,
        jnp.asarray(near),
        jnp.asarray(far),
    )


def solution(mesh):
    placed = (
        P(("sp", "tp"), None),
        P("sp", "tp", None),
        P("sp", "tp", None),
        P("sp", None),
        P("sp", None),
        P(),
        P(None, "tp", None),
        P(None, "tp", None),
        P("tp"),
        P("tp", None),
        P(),
        P("sp", "tp"),
        P("tp", "sp"),
    )
    return jax.shard_map(
        body, mesh=mesh, in_specs=placed, out_specs=P(("sp", "tp"), None), check_vma=False
    )
```

```python
import math

import jax
import jax.numpy as jnp
import numpy as np
from jax import lax
from jax.experimental import pallas as pl
from jax.experimental.pallas import tpu as pltpu
from jax.sharding import PartitionSpec as P

MESH = pl.DeviceIdType.MESH
F32 = jnp.float32
BF16 = jnp.bfloat16

HEADS = 16
NOPE = 128
ROPE = 64
LATENT = 512
VDIM = 128
EPS = 1e-06
THETA = 10000.0

SIDE = 4
BLOCKS = SIDE * SIDE
ROWS = 384
OWN = 48
D = 2048
HID = 1024
PACK = 1152
PAIR = ROWS // 2
EXT = D + 128
UNIT = 1024

UP, UM, VP, VM = (1, 0), (-1, 0), (0, 1), (0, -1)
LINKS = (UP, UM, VP, VM)


def wrap(v):
    return ((v[0] + 4) % 4, (v[1] + 4) % 4)


class Msg:
    def __init__(self, d, e, half, parent):
        self.d, self.e, self.half = d, wrap(e), half
        self.f = wrap((e[0] - d[0], e[1] - d[1]))
        self.level = 1 if parent is None else parent.level + 1
        self.kids = []
        self.id = None


def forwards(m):
    onward = m.d in ((UP, VP) if m.half == 0 else (UM, VM))
    if m.d[1] == 0:
        return ([m.d] if onward and m.f[0] != 2 else []) + [VP, VM]
    return [m.d] if onward and m.f[1] != 2 else []


def build_messages(half):
    todo = [Msg(d, (0, 0), half, None) for d in LINKS]
    done = []
    while todo:
        m = todo.pop(0)
        m.id = half * (BLOCKS - 1) + len(done)
        done.append(m)
        m.kids = [Msg(d, m.f, half, m) for d in forwards(m)]
        todo += m.kids
    return done


TREES = [build_messages(half) for half in (0, 1)]
assert all(sorted({m.f for m in t} | {(0, 0)}) == [(i, j) for i in range(4) for j in range(4)] for t in TREES)
NMSG = 2 * (BLOCKS - 1)
LEVELS = [[[m for m in t if m.level == k] for k in (1, 2, 3, 4)] for t in TREES]
ORDER = [(0, 0)] + [m.f for m in TREES[0]]
SLOT = {f: k for k, f in enumerate(ORDER)}

NEAR = 5
THIRD = PAIR // 6
DIRECT, OVER_X = {}, {}
SHARED = {k: 0 if k < 4 else 1 if k < 11 else 2 if k < 15 else 3 for k in range(1, 16)}
PASSED = {k: 0 if k < 11 else 1 if k < 15 else 2 for k in range(5, 16)}
_row = NEAR * PAIR
for _slots, _table, _rows in (
    (range(5, 11), DIRECT, 4 * THIRD),
    (range(11, 15), DIRECT, 4 * THIRD),
    (range(5, 11), OVER_X, 2 * THIRD),
    (range(15, 16), DIRECT, 4 * THIRD),
    (range(11, 15), OVER_X, 2 * THIRD),
    (range(15, 16), OVER_X, 2 * THIRD),
):
    for _slot in _slots:
        _table[_slot] = _row
        _row += _rows
assert _row == BLOCKS * PAIR

PARTS = ((0, 16), (16, 32), (32, 48), (0, 48))
ALL = len(PARTS) - 1
EDGES = (0, 5, 11, 15, 16)
GROUPS = len(EDGES) - 1


def rotary_tables():
    half = ROPE // 2
    inverse = np.power(THETA, -np.arange(0, ROPE, 2, dtype=np.float64) / ROPE)
    base = inverse[:, None] * np.arange(ROWS)[None, :]
    start = inverse[None, :] * (ROWS * np.arange(BLOCKS))[:, None]
    near = np.concatenate([np.cos(base), np.sin(base)], 0).astype(np.float32)
    far = np.concatenate([np.cos(start), np.sin(start)], 1).astype(np.float32)
    far = np.repeat(far[:, :, None], 128, axis=2)
    assert far.shape == (BLOCKS, 2 * half, 128)
    return near, far


def kernel(
    stream_in,
    qn_in,
    qr_in,
    latent_in,
    kr_in,
    lat_gain_in,
    key_up_in,
    value_up_in,
    out_gain_in,
    out_w_in,
    norm_gain_in,
    ff_in,
    ff_out,
    near_in,
    far_in,
    out,
    lat_gain,
    out_gain,
    norm_gain,
    qn,
    qr_t,
    latent,
    kr_t,
    key_up,
    value_up,
    near,
    cat,
    w1,
    w2,
    qa,
    qb,
    sa,
    sb,
    pa,
    pb,
    acc,
    m_run,
    l_run,
    far,
    stream,
    out_w,
    proj,
    sib,
    xs,
    rx,
    fin,
    act,
    part,
    psib,
    pxs,
    prx,
    mid,
    fsum,
    sums,
    wide,
    wide2,
    er,
    xlr,
    xdr,
    loc_sem,
    ls,
    lr,
    s1,
    r1,
    s2,
    r2,
    dr,
    ps,
    pr,
    fr,
    gr,
):
    sp = lax.axis_index("sp")
    tp = lax.axis_index("tp")
    z, y = sp // SIDE, sp % SIDE
    x, core = tp // 2, tp % 2
    other = 1 - core


    def block_at(dy, dz):
        return ((z + dz) % SIDE) * SIDE + (y + dy) % SIDE

    def at(f):
        return block_at(f[0] * other + f[1] * core, f[0] * core + f[1] * other)

    def torus(d):
        return (at(wrap(d)), tp)

    sibling = (sp, x * 2 + other)

    def across(k):
        return (sp, ((x + k) % SIDE) * 2 + core)

    barrier = pltpu.get_barrier_semaphore()
    peers = [torus(d) for d in LINKS] + [sibling] + [across(k) for k in (1, 2, 3)]
    for peer in peers:
        pl.semaphore_signal(barrier, inc=1, device_id=peer, device_id_type=MESH)

    def local(src, dst, k):
        c = pltpu.make_async_copy(src, dst, loc_sem.at[k])
        c.start()
        return c

    early = [
        local(latent_in, latent, 5),
        local(far_in.at[sp], far, 0),
        local(near_in, near, 6),
        local(kr_in, kr_t, 7),
        local(lat_gain_in, lat_gain, 12),
    ]
    og_copy = local(out_gain_in, out_gain, 13)
    ng_copy = local(norm_gain_in, norm_gain, 14)
    early2 = [local(qn_in, qn, 8), local(key_up_in, key_up, 9), local(qr_in, qr_t, 10)]
    vu_copy = local(value_up_in, value_up, 11)
    w1_copy = local(ff_in, w1.at[sp], 1)
    w2_copy = local(ff_out, w2.at[sp], 2)
    ow_copy = local(out_w_in, out_w, 3)
    st_copy = local(stream_in, stream, 4)

    def remote(src, dst, ssem, rsem, dev):
        return pltpu.make_async_remote_copy(
            src_ref=src, dst_ref=dst, send_sem=ssem, recv_sem=rsem, device_id=dev, device_id_type=MESH
        )

    odd = x % 2

    def lat_rows(start, count):
        return cat.at[pl.ds(pl.multiple_of(start, 32), count), :]

    def lat_view(f, half):
        slot = SLOT[f]
        if slot < NEAR:
            return lat_rows(slot * PAIR + core * 3 * THIRD + (odd + half) * THIRD, THIRD)
        return lat_rows(DIRECT[slot] + core * 2 * THIRD + half * THIRD, THIRD)

    def rest_view(f):
        return lat_rows(SLOT[f] * PAIR + core * 3 * THIRD + (1 - odd) * 2 * THIRD, THIRD)

    def rest_copy(n):
        m = LEVELS[0][0][n]
        return remote(rest_view(m.e), rest_view(m.f), ls.at[0], er.at[0], torus(m.d))

    def in_view(f, half):
        return w1.at[at(f), pl.ds(half * 64, 64), :]

    def in_src(f, half):
        return ff_in.at[pl.ds(half * 64, 64), :] if f == (0, 0) else in_view(f, half)

    def out_view(f, half):
        return w2.at[at(f), pl.ds(half * 512, 512), :]

    def out_src(f, half):
        return ff_out.at[pl.ds(half * 512, 512), :] if f == (0, 0) else out_view(f, half)

    gathers = {
        "L": (lat_view, lat_view, ls, lr),
        "W1": (in_src, in_view, s1, r1),
        "W2": (out_src, out_view, s2, r2),
    }

    def copy_of(g, m):
        src, view, ssem, rsem = gathers[g]
        dst = view(m.f if g == "L" else m.e, m.half)
        k = m.id if g == "L" else m.half * 4 + m.level - 1
        return remote(src(m.e, m.half), dst, ssem.at[0], rsem.at[k], torus(m.d))

    def direct_rows(slot, who):
        if slot < NEAR:
            return lat_rows(slot * PAIR + who * 3 * THIRD, 3 * THIRD)
        return lat_rows(DIRECT[slot] + who * 2 * THIRD, 2 * THIRD)

    def x_rows(slot, who):
        return lat_rows(OVER_X[slot] + who * THIRD, THIRD)

    def share(slot):
        v = direct_rows(slot, core)
        return remote(v, v, ls.at[0], dr.at[SHARED[slot]], sibling)

    def share_x(slot):
        v = x_rows(slot, core)
        return remote(v, v, ls.at[0], xdr.at[PASSED[slot]], sibling)

    def along_x(slot):
        src = lat_rows(DIRECT[slot] + core * 2 * THIRD + odd * THIRD, THIRD)
        to = across(1 if slot % 2 == 0 else 3)
        return remote(src, x_rows(slot, core), ls.at[0], xlr.at[PASSED[slot]], to)

    def await_rows(count, sem):
        v = cat.at[pl.ds(0, count), :]
        remote(v, v, ls.at[0], sem, sibling).wait_recv()

    def pass_over(group):
        slots = [k for k in PASSED if PASSED[k] == group]
        await_rows(THIRD * len(slots), xlr.at[group])
        for slot in slots:
            share_x(slot).start()

    def need(direct, over):
        for group in direct:
            await_rows(
                sum((3 if k < NEAR else 2) * THIRD for k in SHARED if SHARED[k] == group), dr.at[group]
            )
        for group in over:
            await_rows(sum(THIRD for k in PASSED if PASSED[k] == group), xdr.at[group])

    def rest():
        await_rows(len(LINKS) * THIRD, er.at[0])
        for m in LEVELS[0][0]:
            share(SLOT[m.f]).start()

    def begin(g, half):
        for m in LEVELS[half][0]:
            copy_of(g, m).start()

    landed = {}

    def level(g, half, k):
        src, view, ssem, rsem = gathers[g]
        here = LEVELS[half][k - 1]
        if g != "L":
            whole = w1 if g == "W1" else w2
            tall = whole.shape[1] // 2
            if len(here) % 2:
                v = whole.at[0, pl.ds(0, tall), :]
            else:
                v = whole.at[pl.ds(0, len(here) // 2)]
            remote(v, v, ssem.at[0], rsem.at[half * 4 + k - 1], sibling).wait_recv()
        for m in here:
            if g == "L":
                v = view(m.f, half)
                remote(v, v, ssem.at[0], rsem.at[m.id], sibling).wait_recv()
            for kid in m.kids:
                copy_of(g, kid).start()
            if g == "L":
                landed[m.f] = landed.get(m.f, 0) + 1
                if landed[m.f] == 2 and k > 1:
                    along_x(SLOT[m.f]).start()
                    share(SLOT[m.f]).start()

    for c in early:
        c.wait()
    lat = latent[...].astype(F32)
    normed = (
        lat * lax.rsqrt(jnp.mean(lat * lat, axis=-1, keepdims=True) + EPS) * lat_gain[...]
    ).astype(BF16)
    cat[0:PAIR, 0:LATENT] = normed[:PAIR]
    cat[0:PAIR, LATENT + 128 : PACK] = normed[PAIR:]
    half = ROPE // 2
    cos_n, sin_n = near[0:half, :], near[half:ROPE, :]
    cos_f = jnp.broadcast_to(far[0:half, 0:1], (half, ROWS))
    sin_f = jnp.broadcast_to(far[half:ROPE, 0:1], (half, ROWS))
    cosine = cos_n * cos_f - sin_n * sin_f
    sine = sin_n * cos_f + cos_n * sin_f

    def turned(v):
        low, high = v[:half].astype(F32), v[half:].astype(F32)
        a = low * cosine - high * sine
        b = low * sine + high * cosine
        return jnp.transpose(jnp.concatenate([a, b, a, b], axis=0))

    lane = lax.broadcasted_iota(jnp.int32, (ROWS, 128), 1)
    keys = turned(kr_t[...])
    cat[0:PAIR, LATENT : LATENT + 128] = jnp.where(
        lane[:PAIR] < ROPE, keys[:PAIR], keys[PAIR:]
    ).astype(BF16)

    pl.semaphore_wait(barrier, len(peers))
    begin("L", 0)
    begin("L", 1)
    for n in range(len(LINKS)):
        rest_copy(n).start()

    for c in early2:
        c.wait()
    wide[0 : 2 * ROWS, :] = qn[...].astype(F32)
    wide2[...] = key_up[...].astype(F32)
    for h in range(2):
        rows = slice(h * ROWS, (h + 1) * ROWS)
        q_lat = lax.dot_general(
            wide[pl.ds(h, ROWS, stride=2), :].astype(BF16),
            wide2[pl.ds(h, LATENT, stride=2), :].astype(BF16),
            (((1,), (1,)), ((), ())),
            preferred_element_type=F32,
        ).astype(BF16)
        q_rot = turned(qr_t[h])
        qa[rows, 0:LATENT] = q_lat
        qa[rows, LATENT : LATENT + 128] = jnp.where(lane < ROPE, q_rot, 0.0).astype(BF16)
        qb[rows, 128 : LATENT + 128] = q_lat
        qb[rows, 0:128] = jnp.where(lane < ROPE, 0.0, q_rot).astype(BF16)

    acc[...] = jnp.zeros_like(acc)
    m_run[...] = jnp.full_like(m_run, -1e30)
    l_run[...] = jnp.zeros_like(l_run)
    factor = math.log2(math.e) / math.sqrt(NOPE + ROPE)

    def score(q, row, count, first):
        return lax.dot_general(
            q[...],
            cat[row : row + count, first : first + LATENT + 128],
            (((1,), (1,)), ((), ())),
            preferred_element_type=F32,
        )

    def weigh(s_ref, p_ref, row, count, first):
        scores = s_ref[:, 0:count]
        before = m_run[...]
        now = jnp.maximum(before, jnp.max(scores, axis=1, keepdims=True) * factor)
        fade = jnp.exp2(before - now)
        total = l_run[...] * fade
        for k in range(count // 128):
            expo = jnp.exp2(scores[:, k * 128 : (k + 1) * 128] * factor - now)
            total = total + expo
            p_ref[:, k * 128 : (k + 1) * 128] = expo.astype(BF16)
        l_run[...] = total
        m_run[...] = now
        mixed = jnp.dot(
            p_ref[:, 0:count],
            cat[row : row + count, first : first + LATENT],
            preferred_element_type=F32,
        )
        for k in range(LATENT // 128):
            c = slice(k * 128, (k + 1) * 128)
            acc[:, c] = acc[:, c] * fade + mixed[:, c]

    def attend(row, count, between=None):
        sa[:, 0:count] = score(qa, row, count, 0)
        sb[:, 0:count] = score(qb, row, count, LATENT)
        weigh(sa, pa, row, count, 0)
        if between is not None:
            between()
        weigh(sb, pb, row, count, LATENT + 128)

    def last_latents():
        level("L", 0, 4)
        level("L", 1, 4)
        level("W1", 1, 1)

    level("L", 0, 1)
    level("L", 1, 1)
    rest()
    need([0], [])
    attend(0, 768, lambda: begin("W1", 0))
    level("L", 0, 2)
    level("L", 1, 2)
    need([1], [])
    attend(768, 768, lambda: begin("W1", 1))
    level("L", 0, 3)
    level("L", 1, 3)
    level("W1", 0, 1)
    begin("W2", 0)
    pass_over(0)
    need([2], [0])
    attend(1536, 1024, last_latents)
    begin("W2", 1)
    pass_over(1)
    pass_over(2)
    need([3], [1, 2])
    attend(2560, 512, lambda: level("W1", 0, 2))

    out_lat = (acc[...] / jnp.sum(l_run[...], axis=1, keepdims=True)).astype(BF16)
    vu_copy.wait()
    og_copy.wait()
    wide2[...] = value_up[...].astype(F32)
    squares = jnp.zeros((ROWS, 1), F32)
    gated = []
    for h in range(2):
        c = slice(h * VDIM, (h + 1) * VDIM)
        head_out = jnp.dot(
            out_lat[h * ROWS : (h + 1) * ROWS],
            wide2[pl.ds(h, LATENT, stride=2), :].astype(BF16),
            preferred_element_type=F32,
        )
        squares = squares + jnp.sum(head_out * head_out, axis=1, keepdims=True)
        gated.append((head_out * out_gain[:, c]).astype(BF16))
    gated = jnp.concatenate(gated, axis=1)

    def two_terms(total, rows):
        high = total.astype(BF16).astype(F32)
        at_lane = lax.broadcasted_iota(jnp.int32, (rows, 128), 1)
        return jnp.where(at_lane == 0, high, jnp.where(at_lane == 1, total - high, 0.0)).astype(BF16)

    ow_copy.wait()
    tail = two_terms(squares, ROWS)
    for c in range(0, D, 512):
        piece = jnp.dot(gated, out_w[:, c : c + 512], preferred_element_type=F32).astype(BF16)
        proj[:, :, :, c : c + 512] = piece.reshape(SIDE, 2, OWN, 512)
    proj[:, :, :, D:EXT] = tail.reshape(SIDE, 2, OWN, 128)

    def rows_of(p):
        return pl.ds(PARTS[p][0], PARTS[p][1] - PARTS[p][0])

    def swap(p):
        r = rows_of(p)
        return remote(proj.at[:, other, r, :], sib.at[:, r, :], ps.at[0], pr.at[p, 0], sibling)

    def x_copy(p, k):
        r = rows_of(p)
        return remote(xs.at[k - 1, r, :], rx.at[k - 1, r, :], ps.at[1], pr.at[p, 1], across(k))

    def chip_send(p):
        first, last = PARTS[p]
        r = slice(first, last)
        swap(p).wait_recv()
        for k in (2, 1, 3, 0):
            who = (x + k) % SIDE
            both = proj[who, core, r, :].astype(F32) + sib[who, r, :].astype(F32)
            total = jnp.sum(both[:, D:EXT], axis=1, keepdims=True)
            if k:
                xs[k - 1, r, 0:D] = both[:, :D].astype(BF16)
                xs[k - 1, r, D:EXT] = two_terms(total, last - first)
                x_copy(p, k).start()
            else:
                mid[r, :] = both[:, :D]
                sums[r, :] = jnp.broadcast_to(total, (last - first, 128))

    def row_copy(p, k, to, src_tp):
        v = fin.at[src_tp, rows_of(p), :]
        return remote(v, v, ps.at[2], fr.at[p, k if 1 <= k <= 3 else 0], to)

    def came_from(k):
        return ((x + SIDE - k) % SIDE) * 2

    def mid_rows(p):
        r = slice(*PARTS[p])
        projected = mid[r, :]
        total = sums[r, 0:1]
        came = rx.at[:, rows_of(p), :]
        remote(came, came, ps.at[1], pr.at[p, 1], sibling).wait_recv()
        for k in (1, 3, 2):
            projected = projected + rx[k - 1, r, 0:D].astype(F32)
            total = total + jnp.sum(rx[k - 1, r, D:EXT].astype(F32), axis=1, keepdims=True)
        row_scale = lax.rsqrt(total / (HEADS * VDIM) + EPS)
        middle = stream[r, :].astype(F32) + row_scale * projected
        mid[r, :] = middle
        fin[tp, r, :] = (
            middle
            * lax.rsqrt(jnp.mean(middle * middle, axis=-1, keepdims=True) + EPS)
            * norm_gain[...]
        ).astype(BF16)
        for k in (2, 1, 3):
            row_copy(p, k, across(k), tp).start()
        row_copy(p, 0, sibling, tp).start()

    def spread(p):
        for k in (1, 3, 2):
            row_copy(p, k, across(k), came_from(k) + core).wait_recv()
            row_copy(p, 3 + k, sibling, came_from(k) + core).start()

    def spread_end(p):
        v = fin.at[pl.ds(0, SIDE), rows_of(p), :]
        remote(v, v, ps.at[2], fr.at[p, 0], sibling).wait_recv()

    def ff_in_half(p):
        first, last = PARTS[p]
        rows = fin[:, first:last, :].reshape(8 * (last - first), D)
        for c in range(0, HID, 256):
            pre = jnp.dot(
                rows, w1[:, :, c : c + 256].reshape(D, 256), preferred_element_type=F32
            )
            act[8 * first : 8 * last, c : c + 256] = jnp.square(jnp.maximum(pre, 0.0)).astype(BF16)

    def columns_of(g):
        return pl.ds(EDGES[g] * 128, (EDGES[g + 1] - EDGES[g]) * 128)

    def swap_part(g, p):
        r, c = rows_of(p), columns_of(g)
        return remote(
            part.at[:, other, r, c], psib.at[:, r, c], ps.at[3], gr.at[g, p, 0], sibling
        )

    def x_part(g, p, k):
        r, c = rows_of(p), columns_of(g)
        return remote(
            pxs.at[k - 1, r, c], prx.at[k - 1, r, c], ps.at[4], gr.at[g, p, 1], across(k)
        )

    def ff_group(g, p):
        n = EDGES[g]
        while n < EDGES[g + 1]:
            many = min(2, EDGES[g + 1] - n)
            weights = jnp.concatenate([w2[block_at(*ORDER[k])] for k in range(n, n + many)], axis=1)
            first, last = PARTS[p]
            piece = jnp.dot(
                act[8 * first : 8 * last, :], weights, preferred_element_type=F32
            ).astype(BF16)
            for q in range(ALL) if p == ALL else (p,):
                start, stop = PARTS[q]
                rows = piece[8 * (start - first) : 8 * (stop - first)]
                part[:, :, start:stop, n * 128 : (n + many) * 128] = rows.reshape(
                    SIDE, 2, stop - start, many * 128
                )
            n += many
        swap_part(g, p).start()

    def ff_chip(g, p):
        r, c = slice(*PARTS[p]), slice(EDGES[g] * 128, EDGES[g + 1] * 128)
        swap_part(g, p).wait_recv()
        for k in (2, 1, 3, 0):
            who = (x + k) % SIDE
            both = part[who, core, r, c].astype(F32) + psib[who, r, c].astype(F32)
            if k:
                pxs[k - 1, r, c] = both.astype(BF16)
                x_part(g, p, k).start()
            else:
                fsum[r, c] = both

    def ff_end(g, p):
        r = slice(*PARTS[p])
        came = prx.at[:, rows_of(p), columns_of(g)]
        remote(came, came, ps.at[4], gr.at[g, p, 1], sibling).wait_recv()
        for n in range(EDGES[g], EDGES[g + 1]):
            here = slice(n * 128, (n + 1) * 128)
            both = fsum[r, here]
            for k in (1, 3, 2):
                both = both + prx[k - 1, r, here].astype(F32)
            c = pl.ds(pl.multiple_of(block_at(*ORDER[n]) * 128, 128), 128)
            out[r, c] = (mid[r, c] + both).astype(BF16)

    def sent(v, sem):
        remote(v, v, sem, sem, sibling).wait_send()

    for p in range(ALL):
        swap(p).start()
    chip_send(0)
    chip_send(1)
    chip_send(2)
    level("W1", 1, 2)
    level("W2", 0, 1)
    st_copy.wait()
    w1_copy.wait()
    w2_copy.wait()
    ng_copy.wait()
    level("W1", 0, 3)
    level("W2", 1, 1)
    mid_rows(0)
    level("W1", 1, 3)
    mid_rows(1)
    mid_rows(2)
    level("W2", 0, 2)
    spread(0)
    level("W2", 1, 2)
    level("W1", 0, 4)
    level("W1", 1, 4)
    spread_end(0)
    ff_in_half(0)
    ff_group(0, 0)
    spread(1)
    ff_group(1, 0)
    ff_chip(0, 0)
    spread_end(1)
    ff_in_half(1)
    ff_chip(1, 0)
    ff_group(0, 1)
    level("W2", 0, 3)
    spread(2)
    ff_group(1, 1)
    ff_chip(0, 1)
    spread_end(2)
    ff_in_half(2)
    ff_chip(1, 1)
    ff_group(0, 2)
    level("W2", 1, 3)
    ff_group(1, 2)
    ff_chip(0, 2)
    ff_group(2, ALL)
    level("W2", 0, 4)
    ff_chip(1, 2)
    ff_chip(2, ALL)
    level("W2", 1, 4)
    ff_group(3, ALL)
    ff_end(0, 0)
    ff_end(1, 0)
    ff_end(0, 1)
    ff_end(1, 1)
    ff_chip(3, ALL)
    ff_end(0, 2)
    ff_end(1, 2)
    ff_end(2, ALL)
    ff_end(3, ALL)

    tree_rows = 2 * (BLOCKS - 1) * THIRD + len(LINKS) * THIRD
    over_rows = 2 * len(PASSED) * THIRD
    shared_rows = sum((3 if k < NEAR else 2) * THIRD for k in SHARED)
    sent(cat.at[pl.ds(0, tree_rows + over_rows + shared_rows), :], ls.at[0])
    sent(w1.at[pl.ds(0, BLOCKS - 1)], s1.at[0])
    sent(w2.at[pl.ds(0, BLOCKS - 1)], s2.at[0])
    sent(sib, ps.at[0])
    sent(xs, ps.at[1])
    sent(fin.at[pl.ds(0, 2 * SIDE - 1)], ps.at[2])
    sent(psib, ps.at[3])
    sent(pxs, ps.at[4])


def body(
    stream,
    query_nope,
    query_rope,
    latent,
    rope_key,
    latent_gain,
    key_up,
    value_up,
    out_gain,
    out_weight,
    norm_gain,
    ff_in,
    ff_out,
):
    near, far = rotary_tables()
    vmem = pl.BlockSpec(memory_space=pltpu.VMEM)
    hbm = pl.BlockSpec(memory_space=pl.ANY)
    dma = pltpu.SemaphoreType.DMA
    return pl.pallas_call(
        kernel,
        out_shape=jax.ShapeDtypeStruct((OWN, D), BF16),
        in_specs=[hbm] * 15,
        out_specs=vmem,
        scratch_shapes=[
            pltpu.VMEM((1, LATENT), F32),
            pltpu.VMEM((1, 2 * VDIM), F32),
            pltpu.VMEM((1, D), F32),
            pltpu.VMEM((2 * ROWS, NOPE), BF16),
            pltpu.VMEM((2, ROPE, ROWS), BF16),
            pltpu.VMEM((ROWS, LATENT), BF16),
            pltpu.VMEM((ROPE, ROWS), BF16),
            pltpu.VMEM((2 * LATENT, NOPE), BF16),
            pltpu.VMEM((2 * LATENT, VDIM), BF16),
            pltpu.VMEM((ROPE, ROWS), F32),
            pltpu.VMEM((BLOCKS * PAIR, PACK), BF16),
            pltpu.VMEM((BLOCKS, D // BLOCKS, HID), BF16),
            pltpu.VMEM((BLOCKS, HID, D // BLOCKS), BF16),
            pltpu.VMEM((2 * ROWS, LATENT + 128), BF16),
            pltpu.VMEM((2 * ROWS, LATENT + 128), BF16),
            pltpu.VMEM((2 * ROWS, UNIT), F32),
            pltpu.VMEM((2 * ROWS, UNIT), F32),
            pltpu.VMEM((2 * ROWS, UNIT), BF16),
            pltpu.VMEM((2 * ROWS, UNIT), BF16),
            pltpu.VMEM((2 * ROWS, LATENT), F32),
            pltpu.VMEM((2 * ROWS, 128), F32),
            pltpu.VMEM((2 * ROWS, 128), F32),
            pltpu.VMEM((ROPE, 128), F32),
            pltpu.VMEM((OWN, D), BF16),
            pltpu.VMEM((2 * VDIM, D), BF16),
            pltpu.VMEM((SIDE, 2, OWN, EXT), BF16),
            pltpu.VMEM((SIDE, OWN, EXT), BF16),
            pltpu.VMEM((SIDE - 1, OWN, EXT), BF16),
            pltpu.VMEM((SIDE - 1, OWN, EXT), BF16),
            pltpu.VMEM((2 * SIDE, OWN, D), BF16),
            pltpu.VMEM((ROWS, HID), BF16),
            pltpu.VMEM((SIDE, 2, OWN, D), BF16),
            pltpu.VMEM((SIDE, OWN, D), BF16),
            pltpu.VMEM((SIDE - 1, OWN, D), BF16),
            pltpu.VMEM((SIDE - 1, OWN, D), BF16),
            pltpu.VMEM((OWN, D), F32),
            pltpu.VMEM((OWN, D), F32),
            pltpu.VMEM((OWN, 128), F32),
            pltpu.VMEM((2 * ROWS, NOPE), F32),
            pltpu.VMEM((2 * LATENT, NOPE), F32),
            dma((1,)),
            dma((3,)),
            dma((3,)),
            dma((15,)),
            dma((1,)),
            dma((NMSG,)),
            dma((1,)),
            dma((8,)),
            dma((1,)),
            dma((8,)),
            dma((4,)),
            dma((5,)),
            dma((3, 2)),
            dma((3, 4)),
            dma((GROUPS, 4, 2)),
        ],
        compiler_params=pltpu.CompilerParams(
            collective_id=0, has_side_effects=True, vmem_limit_bytes=60 * 1024 * 1024
        ),
    )(
        stream,
        query_nope.reshape(2 * ROWS, NOPE),
        jnp.transpose(query_rope, (1, 2, 0)),
        latent,
        jnp.transpose(rope_key, (1, 0)),
        latent_gain.reshape(1, LATENT),
        key_up.reshape(2 * LATENT, NOPE),
        value_up.reshape(2 * LATENT, VDIM),
        out_gain.reshape(1, 2 * VDIM),
        out_weight,
        norm_gain.reshape(1, D),
        ff_in,
        ff_out,
        jnp.asarray(near),
        jnp.asarray(far),
    )


def solution(mesh):
    placed = (
        P(("sp", "tp"), None),
        P("sp", "tp", None),
        P("sp", "tp", None),
        P("sp", None),
        P("sp", None),
        P(),
        P(None, "tp", None),
        P(None, "tp", None),
        P("tp"),
        P("tp", None),
        P(),
        P("sp", "tp"),
        P("tp", "sp"),
    )
    return jax.shard_map(
        body, mesh=mesh, in_specs=placed, out_specs=P(("sp", "tp"), None), check_vma=False
    )
```
